256 devices in a mesh: sp: 64 (over z, y, core), tp: 4 (over x).
Axes of the slice: x: 4, y: 4, z: 8, core: 2. Of those that a mesh axis runs over, the one named last changes fastest.
Arguments:
- queries: bfloat16 [8192, 1280], P('sp', 'tp'), may hold values from -4000 to 4000
- latents: bfloat16 [8192, 512], P('sp'), may hold values from -6 to 6
- shared_key: bfloat16 [8192, 64], P('sp'), may hold values from -4 to 4
- expand_weight: bfloat16 [512, 1536], P(None, 'tp'), may hold values from -0.25 to 0.25
- residual: bfloat16 [8192, 2048], P('sp'), may hold values from -3 to 3
- out_weight: bfloat16 [768, 2048], replicated, may hold values from -0.21875 to 0.21875
- norm_gain: bfloat16 [2048], replicated, may hold values from 0.099609375 to 1.8984375
- gate_weight: bfloat16 [2048, 3072], P('sp', 'tp'), may hold values from -0.125 to 0.125
- value_weight: bfloat16 [2048, 3072], P('sp', 'tp'), may hold values from -0.125 to 0.125
- conv_weight: bfloat16 [3, 3072], P(None, 'tp'), may hold values from -3.5 to 3.5
- down_weight: bfloat16 [3072, 2048], P('tp', 'sp'), may hold values from -0.109375 to 0.109375
Outputs:
- output: bfloat16 [8192, 2048], P(('sp', 'tp'))
The draws below stay inside these ranges and needn't reach their ends.
All inputs are finite; a program needn't handle non-finite values.
Results may differ from the reference program's by a relative error of at most 0.018.
Values may be sent and summed in bfloat16 or wider, within the bound.
No kernel may reach another device: no remote copies, remote signals or barrier semaphores. Data moves between devices by JAX's collectives and lax.ppermute only.
A program may use at most 128 MiB of HBM per device.

```python
import jax
import jax.numpy as jnp
from jax import lax

D = 2048
HEADS = 4
NOPE_A = 128
VAL_A = 128
NOPE_B = 64
VAL_B = 64
ROPE = 64
RANK = 512
FF = 3072
CONV = 3
TOK_DEV = 128
TOKENS = 8192


def shared_rows(key):
    drawn = jax.random.normal(jax.random.fold_in(key, 11), (TOKENS, ROPE), jnp.float32)
    return jnp.clip(drawn, -4.0, 4.0).astype(jnp.float32)


def draw_shared_key(key, part):
    return shared_rows(key).reshape(TOKENS, ROPE).astype(jnp.bfloat16)


def draw_queries(key, part):
    q_width = NOPE_A + NOPE_B + 2 * ROPE
    base_draw = jnp.clip(3.0 * jax.random.normal(jax.random.fold_in(key, 23), (TOKENS, HEADS, q_width), jnp.float32), -18.0, 18.0)
    return jnp.clip(base_draw, -4000.0, 4000.0).reshape(TOKENS, HEADS * q_width).astype(jnp.bfloat16)


def steps_of(own_key, extent, pieces, low, high):
    gain, own = 1.0, jax.random.fold_in(own_key, 6)
    for dim, parts in pieces:
        heights = jnp.exp(jax.random.uniform(jax.random.fold_in(own, dim), (parts,), jnp.float32, low / len(pieces), high / len(pieces)))
        gain = gain * jnp.repeat(heights, extent[dim] // parts).reshape([-1 if axis == dim else 1 for axis in range(len(extent))])
    return gain


def noise(stream_key, shape, deviation, limit, pieces=(), held_as=jnp.bfloat16):
    array = jax.random.normal(stream_key, shape, jnp.float32) * deviation
    if len(pieces) > 0:
        array = steps_of(stream_key, shape, pieces, -0.22, 0.18) * array
    return jnp.clip(array, min=-limit, max=limit).astype(held_as)


def setup_inputs(seed: int = 0) -> dict:
    key_of = jax.random.split(jax.random.key(seed), 12)
    return {
        "queries": draw_queries(jax.random.fold_in(key_of[11], 71), 0),
        "latents": noise(key_of[1], (TOKENS, RANK), 1.0, 6.0, ((0, 64),)),
        "shared_key": draw_shared_key(jax.random.fold_in(key_of[11], 71), 0),
        "expand_weight": noise(key_of[3], (RANK, HEADS * (NOPE_A + VAL_A + NOPE_B + VAL_B)), RANK ** -0.5, 0.25, ((1, 4),)),
        "residual": noise(key_of[4], (TOKENS, D), 0.5, 3.0, ((0, 64),)),
        "out_weight": noise(key_of[5], (HEADS * (VAL_A + VAL_B), D), (HEADS * (VAL_A + VAL_B)) ** -0.5, 0.21875),
        "norm_gain": jnp.clip(1.0 + 0.18 * jax.random.normal(key_of[6], (D,), jnp.float32), 0.099609375, 1.8984375).astype(jnp.bfloat16),
        "gate_weight": noise(key_of[7], (D, FF), D ** -0.5, 0.125, ((0, 64), (1, 4))),
        "value_weight": noise(key_of[8], (D, FF), D ** -0.5, 0.125, ((0, 64), (1, 4))),
        "conv_weight": noise(key_of[9], (CONV, FF), CONV ** -0.5, 3.5, ((1, 4),)),
        "down_weight": noise(key_of[10], (FF, D), FF ** -0.5, 0.109375, ((0, 4), (1, 64))),
    }


def tables(positions, width):
    half_width = width // 2
    frequency = 10000.0 ** (-jnp.arange(half_width, dtype=jnp.float32) / half_width)
    angles = positions.astype(jnp.float32)[:, None] * frequency[None, :]
    return (jnp.cos(angles), jnp.sin(angles))

def rotate(vectors, cos_table, sine_table):
    half_width = vectors.shape[-1] // 2
    first_half = vectors[:, :half_width].astype(jnp.float32)
    second_half = vectors[:, half_width:].astype(jnp.float32)
    turned = jnp.concatenate([first_half * cos_table - second_half * sine_table, second_half * cos_table + first_half * sine_table], axis=1)
    return turned.astype(jnp.bfloat16)

def attend_head(q_content, q_turned, k_content, k_turned, values, score_scale):
    tokens = q_content.shape[0]
    blocks = tokens // TOK_DEV

    def one_block(block_index):
        first_row = (block_index * TOK_DEV).astype(jnp.int32)
        content = lax.dynamic_slice_in_dim(q_content, first_row, TOK_DEV, 0)
        rotary = lax.dynamic_slice_in_dim(q_turned, first_row, TOK_DEV, 0)
        scores = (jnp.dot(content, k_content.T, preferred_element_type=jnp.float32) + jnp.dot(rotary, k_turned.T, preferred_element_type=jnp.float32)) * score_scale
        row_max = lax.optimization_barrier(jnp.max(scores, axis=1, keepdims=True))
        weights = jnp.exp(scores - row_max)
        row_sum = lax.optimization_barrier(jnp.sum(weights, axis=1, keepdims=True))
        weighted = jnp.dot(weights.astype(jnp.bfloat16), values, preferred_element_type=jnp.float32)
        return (weighted / row_sum).astype(jnp.bfloat16)
    result = lax.map(one_block, jnp.arange(blocks, dtype=jnp.int32))
    return result.reshape(tokens, values.shape[1])

def reference(queries, latents, shared_key, expand_weight, residual, out_weight, norm_gain, gate_weight, value_weight, conv_weight, down_weight):
    tokens = queries.shape[0]
    q_width = NOPE_A + NOPE_B + 2 * ROPE
    kv_width = NOPE_A + VAL_A + NOPE_B + VAL_B
    cos_table, sine_table = tables(jnp.arange(tokens, dtype=jnp.int32), ROPE)
    key_turned = rotate(shared_key, cos_table, sine_table)
    expanded = jnp.dot(latents, expand_weight, preferred_element_type=jnp.float32).astype(jnp.bfloat16)
    scale_wide = (NOPE_A + ROPE) ** (-0.5)
    scale_narrow = (NOPE_B + ROPE) ** (-0.5)
    outputs = []
    for pair_index in range(HEADS):
        q_base = pair_index * q_width
        kv_base = pair_index * kv_width
        wide_content = queries[:, q_base:q_base + NOPE_A]
        narrow_content = queries[:, q_base + NOPE_A:q_base + NOPE_A + NOPE_B]
        rotary_base = q_base + NOPE_A + NOPE_B
        wide_turned = rotate(queries[:, rotary_base:rotary_base + ROPE], cos_table, sine_table)
        narrow_turned = rotate(queries[:, rotary_base + ROPE:rotary_base + 2 * ROPE], cos_table, sine_table)
        wide_keys = expanded[:, kv_base:kv_base + NOPE_A]
        wide_values = expanded[:, kv_base + NOPE_A:kv_base + NOPE_A + VAL_A]
        narrow_base = kv_base + NOPE_A + VAL_A
        narrow_keys = expanded[:, narrow_base:narrow_base + NOPE_B]
        narrow_values = expanded[:, narrow_base + NOPE_B:narrow_base + NOPE_B + VAL_B]
        outputs.append(attend_head(wide_content, wide_turned, wide_keys, key_turned, wide_values, scale_wide))
        outputs.append(attend_head(narrow_content, narrow_turned, narrow_keys, key_turned, narrow_values, scale_narrow))
    attended = jnp.concatenate(outputs, axis=1)
    projected = jnp.dot(attended, out_weight, preferred_element_type=jnp.float32)
    stream = (residual.astype(jnp.float32) + projected).astype(jnp.bfloat16)
    stream_f = stream.astype(jnp.float32)
    scaled = stream_f * lax.rsqrt(lax.optimization_barrier(jnp.mean(stream_f * stream_f, axis=1, keepdims=True)) + 1e-06)
    normed = (scaled * norm_gain.astype(jnp.float32)).astype(jnp.bfloat16)
    gate_pre = jnp.dot(normed, gate_weight, preferred_element_type=jnp.float32).astype(jnp.bfloat16)
    value_pre = jnp.dot(normed, value_weight, preferred_element_type=jnp.float32).astype(jnp.bfloat16)
    reach = CONV // 2
    padded = jnp.pad(gate_pre, ((reach, reach), (0, 0)))
    mixed_gate = jnp.zeros(gate_pre.shape, jnp.float32)
    for tap in range(CONV):
        mixed_gate = mixed_gate + padded[tap:tap + tokens].astype(jnp.float32) * conv_weight[tap].astype(jnp.float32)
    active = (jax.nn.silu(mixed_gate) * value_pre.astype(jnp.float32)).astype(jnp.bfloat16)
    down = jnp.dot(active, down_weight, preferred_element_type=jnp.float32)
    return (stream.astype(jnp.float32) + down).astype(jnp.bfloat16)
```

```python
import functools

import jax
import jax.numpy as jnp
from jax import lax
from jax.experimental import pallas as pl
from jax.experimental.pallas import tpu as pltpu
from jax.sharding import Mesh
from jax.sharding import PartitionSpec as P

NOPE_A = 128
VAL_A = 128
NOPE_B = 64
VAL_B = 64
ROPE = 64
Z, Y, C, X = 8, 4, 2, 4
SP = ("z", "y", "c")
SP_TP = ("z", "y", "c", "x")
LOG2E = 1.4426950408889634
ROWS = 144
BF = jnp.bfloat16
F32 = jnp.float32


def shift(x, axis, k):
    n = lax.axis_size(axis)
    return lax.ppermute(x, axis, [(i, (i + k) % n) for i in range(n)])


def swap(x):
    return lax.ppermute(x, "c", [(0, 1), (1, 0)])


def after(x, *deps):
    return lax.optimization_barrier((x, *deps))[0]


def tables(positions, width):
    half_width = width // 2
    frequency = 10000.0 ** (-jnp.arange(half_width, dtype=F32) / half_width)
    angles = positions.astype(F32)[:, None] * frequency[None, :]
    return (jnp.cos(angles), jnp.sin(angles))


def rotate(vectors, cos_table, sine_table):
    half_width = vectors.shape[-1] // 2
    a = vectors[:, :half_width].astype(F32)
    b = vectors[:, half_width:].astype(F32)
    turned = jnp.concatenate(
        [a * cos_table - b * sine_table, b * cos_table + a * sine_table], axis=1
    )
    return turned.astype(BF)


def split3(v):
    hi = v.astype(BF)
    r = v - hi.astype(F32)
    mid = r.astype(BF)
    lo = (r - mid.astype(F32)).astype(BF)
    return [hi.astype(F32), mid.astype(F32), lo.astype(F32)]


def attend_kernel(nq, nk, *refs):
    qs, ks, outs = refs[:nq], refs[nq : nq + nk], refs[nq + nk :]
    keys = jnp.concatenate([k[:, 0:256] for k in ks], axis=0)
    values = jnp.concatenate([k[:, 256:512] for k in ks], axis=0)
    cw = float((NOPE_A + ROPE) ** -0.5 * LOG2E)
    cn = float((NOPE_B + ROPE) ** -0.5 * LOG2E)
    nt = (((1,), (1,)), ((), ()))
    lane = lax.broadcasted_iota(jnp.int32, (ROWS, 128), 1)
    for q, o in zip(qs, outs):
        sw = lax.dot_general(q[:, 0:256], keys, nt, preferred_element_type=F32)
        mw = jnp.max(sw, axis=1, keepdims=True)
        pw = jnp.exp2((sw - mw) * cw).astype(BF)
        ow = jnp.dot(pw, values, preferred_element_type=F32)
        sn = lax.dot_general(q[:, 256:384], keys[:, 128:256], nt, preferred_element_type=F32)
        mn = jnp.max(sn, axis=1, keepdims=True)
        pn = jnp.exp2((sn - mn) * cn).astype(BF)
        on = jnp.dot(pn, values[:, 128:256], preferred_element_type=F32)
        lw = ow[:, 192:193]
        ln = on[:, 64:65]
        second = on / ln
        pieces = split3(mw * cw) + split3(lw) + split3(mn * cn) + split3(ln)
        for at, piece in enumerate(pieces):
            second = jnp.where(lane == 64 + at, piece, second)
        o[:, 0:128] = (ow[:, 0:128] / lw).astype(BF)
        o[:, 128:256] = second.astype(BF)


def attend(q_blocks, k_blocks):
    nq, nk = len(q_blocks), len(k_blocks)
    return pl.pallas_call(
        functools.partial(attend_kernel, nq, nk),
        out_shape=[jax.ShapeDtypeStruct((ROWS, 256), BF)] * nq,
        name="attend",
    )(*q_blocks, *k_blocks)


def join_kernel(*refs):
    parts, out = refs[:-1], refs[-1]
    seconds = [p[:, 128:256].astype(F32) for p in parts]

    def stat(at):
        return [s[:, at : at + 1] + s[:, at + 1 : at + 2] + s[:, at + 2 : at + 3] for s in seconds]

    def weights(ms, ls):
        top = functools.reduce(jnp.maximum, ms)
        ws = [jnp.exp2(m - top) * l for m, l in zip(ms, ls)]
        total = functools.reduce(jnp.add, ws)
        return [w / total for w in ws]

    ww = weights(stat(64), stat(67))
    wn = weights(stat(70), stat(73))
    wide = functools.reduce(jnp.add, [w * p[:, 0:128].astype(F32) for w, p in zip(ww, parts)])
    narrow = functools.reduce(jnp.add, [w * s for w, s in zip(wn, seconds)])
    lane = lax.broadcasted_iota(jnp.int32, (ROWS, 128), 1)
    out[:, 0:128] = wide.astype(BF)
    out[:, 128:256] = jnp.where(lane < 64, narrow, 0.0).astype(BF)


def join(parts):
    return pl.pallas_call(
        join_kernel, out_shape=jax.ShapeDtypeStruct((ROWS, 256), BF), name="join"
    )(*parts)


def project_kernel(meta, *refs):
    parts = refs[:X]
    out_weight, residual, halo, gain, stream_own, normed, stream = refs[X:]
    x = meta[0]
    total = None
    for k, part in enumerate(parts):
        first = pl.multiple_of(lax.rem(x + k, X) * 192, 64)
        d = jnp.dot(part[:, 0:192], out_weight[pl.ds(first, 192), :], preferred_element_type=F32)
        total = d if total is None else total + d
    res = jnp.concatenate([residual[...], halo[...]], axis=0).astype(F32)
    s = (res + total).astype(BF)
    stream[...] = s
    s = s.astype(F32)
    n = s * lax.rsqrt(jnp.mean(s * s, axis=1, keepdims=True) + 1e-06) * gain[...].astype(F32)
    row = lax.broadcasted_iota(jnp.int32, (ROWS, 1), 0)
    n = jnp.where(row < 128 + meta[1], n, 0.0)
    normed[...] = n.astype(BF)
    stream_own[...] = stream[pl.ds(pl.multiple_of(x * 32, 32), 32), :]


def project(meta, parts, out_weight, residual, halo, gain):
    vmem = pl.BlockSpec(memory_space=pltpu.VMEM)
    return pl.pallas_call(
        project_kernel,
        in_specs=[pl.BlockSpec(memory_space=pltpu.SMEM)] + [vmem] * 8,
        out_shape=[
            jax.ShapeDtypeStruct((32, 2048), BF),
            jax.ShapeDtypeStruct((ROWS, 2048), BF),
        ],
        scratch_shapes=[pltpu.VMEM((ROWS, 2048), BF)],
        name="project",
    )(meta, *parts, out_weight, residual, halo, gain)


def mixer_kernel(offsets, meta, own, other, taps, *refs):
    n = len(offsets)
    ws, (keep, send) = refs[:n], refs[n:]
    z, c = meta[2], meta[3]
    acc = None
    for w, off in zip(ws, offsets):
        cols = pl.ds(pl.multiple_of(lax.rem(z + off, Z) * 256, 256), 256)
        lhs = jnp.concatenate([own[:, cols], other[:, cols]], axis=0)
        d = jnp.dot(lhs, w[:, 0:768], preferred_element_type=F32)
        acc = d if acc is None else acc + d
    pre = acc.astype(BF).astype(F32)
    gate, value = pre[:, 0:384], pre[:, 384:768]
    ga, gb = gate[0:128], gate[ROWS : ROWS + 128]
    ha, hb = gate[128:129], gate[ROWS + 128 : ROWS + 129]
    va, vb = value[0:128], value[ROWS : ROWS + 128]
    t0 = taps[0:1, :].astype(F32)
    t1 = taps[1:2, :].astype(F32)
    t2 = taps[2:3, :].astype(F32)
    row = lax.broadcasted_iota(jnp.int32, (128, 1), 0)
    low = c == 0

    def mixed(g, before, behind, v):
        prev = jnp.where(row == 0, before, pltpu.roll(g, 1, 0))
        nxt = jnp.where(row == 127, behind, pltpu.roll(g, 127, 0))
        m = prev * t0 + g * t1 + nxt * t2
        return (m / (1.0 + jnp.exp(-m)) * v).astype(BF)

    aa = mixed(ga, jnp.where(low, ha, gb[127:128]), jnp.where(low, gb[0:1], ha), va)
    ab = mixed(gb, jnp.where(low, ga[127:128], hb), jnp.where(low, hb, ga[0:1]), vb)
    act = jnp.concatenate([aa, ab], axis=0)
    for w, off in zip(ws, offsets):
        cols = pl.ds(pl.multiple_of(lax.rem(z + off, Z) * 256, 256), 256)
        d = lax.dot_general(
            act, w[:, 768:1152], (((1,), (1,)), ((), ())), preferred_element_type=F32
        )
        keep[:, cols] = d[0:128]
        send[:, cols] = d[128:256].astype(BF)


def mixer(meta, own, other, taps, offsets, ws):
    vmem = pl.BlockSpec(memory_space=pltpu.VMEM)
    return pl.pallas_call(
        functools.partial(mixer_kernel, offsets),
        in_specs=[pl.BlockSpec(memory_space=pltpu.SMEM)] + [vmem] * (3 + len(ws)),
        out_shape=[
            jax.ShapeDtypeStruct((128, 2048), F32),
            jax.ShapeDtypeStruct((128, 2048), BF),
        ],
        name="mixer",
    )(meta, own, other, taps, *ws)


def body(
    queries,
    latents,
    shared_key,
    expand_weight,
    residual,
    out_weight,
    norm_gain,
    gate_weight,
    value_weight,
    conv_weight,
    down_weight,
):
    z, y, c, x = (lax.axis_index(a) for a in ("z", "y", "c", "x"))
    s = lax.axis_index(SP)
    tok = queries.shape[0]
    lat2 = jnp.concatenate([latents, swap(latents)], axis=0)
    sk2 = jnp.concatenate([shared_key, swap(shared_key)], axis=0)
    own_pos = s * tok + jnp.arange(tok, dtype=jnp.int32)
    other_pos = (s + 1 - 2 * c) * tok + jnp.arange(tok, dtype=jnp.int32)
    cos2, sin2 = tables(jnp.concatenate([own_pos, other_pos]), ROPE)
    cos, sin = cos2[:tok], sin2[:tok]
    ew = expand_weight
    expanded = jnp.dot(lat2, ew, preferred_element_type=F32).astype(BF)
    turned = rotate(sk2, cos2, sin2)
    ones = jnp.broadcast_to(
        (jnp.arange(64) == 0).astype(BF)[None, :], (2 * tok, 64)
    )
    kv = jnp.concatenate(
        [
            expanded[:, 0:128],
            turned,
            expanded[:, 256:320],
            expanded[:, 128:256],
            expanded[:, 320:384],
            ones,
        ],
        axis=1,
    )
    rot0 = NOPE_A + NOPE_B
    q = jnp.concatenate(
        [
            queries[:, 0:128],
            rotate(queries[:, rot0 : rot0 + 64], cos, sin),
            jnp.zeros((tok, 64), BF),
            rotate(queries[:, rot0 + 64 : rot0 + 128], cos, sin),
            queries[:, 128:192],
        ],
        axis=1,
    )
    nsp = Z * Y * C
    pairs = [(i, i + 1) for i in range(1, nsp - 1, 2)] + [(i, i - 1) for i in range(2, nsp, 2)]
    edge = jnp.concatenate([q, residual], axis=1)
    edge = jnp.where(c == 1, edge[tok - 1 : tok], edge[0:1])
    edge = lax.ppermute(edge, SP, pairs)
    edge = jnp.pad(edge, ((0, 15), (0, 0)))
    q = jnp.concatenate([q, edge[:, :384]], axis=0)
    halo_res = edge[:, 384:]
    def halves(w, axis):
        n = w.shape[axis] // 2
        lo = lax.slice_in_dim(w, 0, n, axis=axis)
        hi = lax.slice_in_dim(w, n, 2 * n, axis=axis)
        return jnp.where(c == 0, lo, hi), jnp.where(c == 0, hi, lo)

    gk, gs = halves(gate_weight, 1)
    vk, vs = halves(value_weight, 1)
    dk, ds = halves(down_weight.T, 1)
    wk = jnp.concatenate([gk, vk, dk], axis=1)
    wr = swap(jnp.concatenate([gs, vs, ds], axis=1))
    w = jnp.concatenate([jnp.where(c == 0, wk, wr), jnp.where(c == 0, wr, wk)], axis=0)
    q_blocks = [q] + [shift(q, "y", k) for k in (1, 2, 3)]
    wf = shift(w, "y", 1)
    wb = shift(w, "y", -1)
    wo = jnp.concatenate([shift(wf[:32], "y", 1), shift(wb[32:], "y", -1)], axis=0)
    stack = jnp.concatenate([w, wb, wo, wf], axis=0)
    stack = jnp.concatenate([stack, stack], axis=0)
    w = lax.dynamic_slice_in_dim(stack, lax.rem(Y - y, Y) * 64, 256, 0)
    ring = [(2 * i, 2 * ((i + 1) % Z)) for i in range(Z)]
    ring += [(2 * i + 1, 2 * ((i - 1) % Z) + 1) for i in range(Z)]
    r1 = lax.ppermute(kv, ("z", "c"), ring)
    r2 = lax.ppermute(r1, ("z", "c"), ring)
    r3 = lax.ppermute(r2, ("z", "c"), ring)
    r4 = lax.ppermute(r3[:tok], ("z", "c"), ring)
    k_blocks = [kv, r1, swap(r1), r2, swap(r2), r3, swap(r3), r4, swap(r4)]
    f1, b1 = shift(w, "z", 1), shift(w, "z", -1)
    f2, b2 = shift(f1, "z", 1), shift(b1, "z", -1)
    f3, b3 = shift(f2, "z", 1), shift(b2, "z", -1)
    o4 = jnp.concatenate([shift(f3[:128], "z", 1), shift(b3[128:], "z", -1)], axis=0)
    offsets = (0, 7, 1, 6, 2, 5, 3, 4)
    ws = [w, f1, b1, f2, b2, f3, b3, o4]
    o = attend(q_blocks, k_blocks)
    parts = [o[0]] + [shift(o[k], "y", -k) for k in (1, 2, 3)]
    attended = join(parts)
    heads = [attended] + [shift(attended, "x", -k) for k in (1, 2, 3)]
    valid = jnp.where(c == 0, s > 0, s < nsp - 1).astype(jnp.int32)
    meta = jnp.stack([x, valid, z, c]).astype(jnp.int32)
    stream_own, normed = project(
        meta, heads, out_weight, residual, halo_res, norm_gain.reshape(1, -1)
    )
    other = swap(normed)
    taps = jnp.where(c == 0, conv_weight[:, :384], conv_weight[:, 384:])
    keep, send = mixer(meta, normed, other, taps, offsets, ws)
    total = keep + swap(send).astype(F32)
    tb = total.astype(BF)
    got = []
    for k in (1, 2, 3):
        piece = lax.dynamic_slice_in_dim(tb, lax.rem(x + k, X) * 32, 32, 0)
        got.append(shift(piece, "x", k))
    mine = lax.dynamic_slice_in_dim(total, x * 32, 32, 0)
    summed = mine + got[0].astype(F32) + got[1].astype(F32) + got[2].astype(F32)
    return (stream_own.astype(F32) + summed).astype(BF)


def solution(mesh):
    split = Mesh(mesh.devices.reshape(Z, Y, C, X), SP_TP)
    placed = (
        P(SP, "x"),
        P(SP, None),
        P(SP, None),
        P(None, "x"),
        P(SP, None),
        P(),
        P(),
        P(SP, "x"),
        P(SP, "x"),
        P(None, "x"),
        P("x", SP),
    )
    return jax.shard_map(
        body, mesh=split, in_specs=placed, out_specs=P(SP_TP, None), check_vma=False
    )
```

```python
import functools

import jax
import jax.numpy as jnp
from jax import lax
from jax.experimental import pallas as pl
from jax.experimental.pallas import tpu as pltpu
from jax.sharding import Mesh
from jax.sharding import PartitionSpec as P

NOPE_A = 128
VAL_A = 128
NOPE_B = 64
VAL_B = 64
ROPE = 64
Z, Y, C, X = 8, 4, 2, 4
SP = ("z", "y", "c")
SP_TP = ("z", "y", "c", "x")
LOG2E = 1.4426950408889634
ROWS = 144
BF = jnp.bfloat16
F32 = jnp.float32


def limit(mib):
    return pltpu.CompilerParams(vmem_limit_bytes=mib * 1024 * 1024)


def shift(x, axis, k):
    n = lax.axis_size(axis)
    return lax.ppermute(x, axis, [(i, (i + k) % n) for i in range(n)])


def swap(x):
    return lax.ppermute(x, "c", [(0, 1), (1, 0)])


def after(x, *deps):
    return lax.optimization_barrier((x, *deps))[0]


def tables(positions, width):
    half_width = width // 2
    frequency = 10000.0 ** (-jnp.arange(half_width, dtype=F32) / half_width)
    angles = positions.astype(F32)[:, None] * frequency[None, :]
    return (jnp.cos(angles), jnp.sin(angles))


def rotate(vectors, cos_table, sine_table):
    half_width = vectors.shape[-1] // 2
    a = vectors[:, :half_width].astype(F32)
    b = vectors[:, half_width:].astype(F32)
    turned = jnp.concatenate(
        [a * cos_table - b * sine_table, b * cos_table + a * sine_table], axis=1
    )
    return turned.astype(BF)


def split3(v):
    hi = v.astype(BF)
    r = v - hi.astype(F32)
    mid = r.astype(BF)
    lo = (r - mid.astype(F32)).astype(BF)
    return [hi.astype(F32), mid.astype(F32), lo.astype(F32)]


def attend_kernel(nq, nk, *refs):
    qs, ks, outs = refs[:nq], refs[nq : nq + nk], refs[nq + nk :]
    keys = jnp.concatenate([k[:, 0:256] for k in ks], axis=0)
    values = jnp.concatenate([k[:, 256:512] for k in ks], axis=0)
    cw = float((NOPE_A + ROPE) ** -0.5 * LOG2E)
    cn = float((NOPE_B + ROPE) ** -0.5 * LOG2E)
    nt = (((1,), (1,)), ((), ()))
    lane = lax.broadcasted_iota(jnp.int32, (ROWS, 128), 1)
    for q, o in zip(qs, outs):
        sw = lax.dot_general(q[:, 0:256], keys, nt, preferred_element_type=F32)
        mw = jnp.max(sw, axis=1, keepdims=True)
        pw = jnp.exp2((sw - mw) * cw).astype(BF)
        ow = jnp.dot(pw, values, preferred_element_type=F32)
        sn = lax.dot_general(q[:, 256:384], keys[:, 128:256], nt, preferred_element_type=F32)
        mn = jnp.max(sn, axis=1, keepdims=True)
        pn = jnp.exp2((sn - mn) * cn).astype(BF)
        on = jnp.dot(pn, values[:, 128:256], preferred_element_type=F32)
        lw = ow[:, 192:193]
        ln = on[:, 64:65]
        second = on / ln
        pieces = split3(mw * cw) + split3(lw) + split3(mn * cn) + split3(ln)
        for at, piece in enumerate(pieces):
            second = jnp.where(lane == 64 + at, piece, second)
        o[:, 0:128] = (ow[:, 0:128] / lw).astype(BF)
        o[:, 128:256] = second.astype(BF)


def attend(q_blocks, k_blocks):
    nq, nk = len(q_blocks), len(k_blocks)
    return pl.pallas_call(
        functools.partial(attend_kernel, nq, nk),
        out_shape=[jax.ShapeDtypeStruct((ROWS, 256), BF)] * nq,
        name="attend", compiler_params=limit(24),
    )(*q_blocks, *k_blocks)


def join_kernel(*refs):
    parts, out = refs[:-1], refs[-1]
    seconds = [p[:, 128:256].astype(F32) for p in parts]

    def stat(at):
        return [s[:, at : at + 1] + s[:, at + 1 : at + 2] + s[:, at + 2 : at + 3] for s in seconds]

    def weights(ms, ls):
        top = functools.reduce(jnp.maximum, ms)
        ws = [jnp.exp2(m - top) * l for m, l in zip(ms, ls)]
        total = functools.reduce(jnp.add, ws)
        return [w / total for w in ws]

    ww = weights(stat(64), stat(67))
    wn = weights(stat(70), stat(73))
    wide = functools.reduce(jnp.add, [w * p[:, 0:128].astype(F32) for w, p in zip(ww, parts)])
    narrow = functools.reduce(jnp.add, [w * s for w, s in zip(wn, seconds)])
    lane = lax.broadcasted_iota(jnp.int32, (ROWS, 128), 1)
    out[:, 0:128] = wide.astype(BF)
    out[:, 128:256] = jnp.where(lane < 64, narrow, 0.0).astype(BF)


def join(parts):
    return pl.pallas_call(
        join_kernel, out_shape=jax.ShapeDtypeStruct((ROWS, 256), BF), name="join", compiler_params=limit(4)
    )(*parts)


def project_kernel(meta, *refs):
    parts = refs[:X]
    out_weight, residual, halo, gain, stream_own, normed, stream = refs[X:]
    x = meta[0]
    total = None
    for k, part in enumerate(parts):
        first = pl.multiple_of(lax.rem(x + k, X) * 192, 64)
        d = jnp.dot(part[:, 0:192], out_weight[pl.ds(first, 192), :], preferred_element_type=F32)
        total = d if total is None else total + d
    res = jnp.concatenate([residual[...], halo[...]], axis=0).astype(F32)
    s = (res + total).astype(BF)
    stream[...] = s
    s = s.astype(F32)
    n = s * lax.rsqrt(jnp.mean(s * s, axis=1, keepdims=True) + 1e-06) * gain[...].astype(F32)
    row = lax.broadcasted_iota(jnp.int32, (ROWS, 1), 0)
    n = jnp.where(row < 128 + meta[1], n, 0.0)
    normed[...] = n.astype(BF)
    stream_own[...] = stream[pl.ds(pl.multiple_of(x * 32, 32), 32), :]


def project(meta, parts, out_weight, residual, halo, gain):
    vmem = pl.BlockSpec(memory_space=pltpu.VMEM)
    return pl.pallas_call(
        project_kernel,
        in_specs=[pl.BlockSpec(memory_space=pltpu.SMEM)] + [vmem] * 8,
        out_shape=[
            jax.ShapeDtypeStruct((32, 2048), BF),
            jax.ShapeDtypeStruct((ROWS, 2048), BF),
        ],
        scratch_shapes=[pltpu.VMEM((ROWS, 2048), BF)],
        name="project", compiler_params=limit(16),
    )(meta, *parts, out_weight, residual, halo, gain)


def mixer_kernel(meta, own, other, taps, *refs):
    n = len(OFFSETS)
    ws, downs, (keep, send, down) = refs[:n], refs[n:-3], refs[-3:]
    z, c, y = meta[2], meta[3], meta[4]
    acc = None
    for w, off in zip(ws, OFFSETS):
        cols = pl.ds(pl.multiple_of(lax.rem(z + off, Z) * 256, 256), 256)
        lhs = jnp.concatenate([own[:, cols], other[:, cols]], axis=0)
        d = jnp.dot(lhs, w[...], preferred_element_type=F32)
        acc = d if acc is None else acc + d
    sign = 2 * c - 1
    for dy, part in enumerate(downs):
        yy = lax.rem(y + dy, Y)

        def put(first, count, zz, extra):
            at = pl.multiple_of((lax.rem(zz + 2 * Z, Z) * Y + yy) * 64 + extra, 32)
            down[pl.ds(at, count), :] = part[first : first + count, :]

        put(0, 64, z, 0)
        for k in (1, 2, 3):
            put(64 * k, 64, z + sign * k, 0)
            put(224 + 64 * k, 64, z - sign * k, 0)
        put(256, 32, z + 4, 32 * c)
        put(480, 32, z + 4, 32 - 32 * c)
    pre = acc.astype(BF).astype(F32)
    gate, value = pre[:, 0:384], pre[:, 384:768]
    ga, gb = gate[0:128], gate[ROWS : ROWS + 128]
    ha, hb = gate[128:129], gate[ROWS + 128 : ROWS + 129]
    va, vb = value[0:128], value[ROWS : ROWS + 128]
    t0 = taps[0:1, :].astype(F32)
    t1 = taps[1:2, :].astype(F32)
    t2 = taps[2:3, :].astype(F32)
    row = lax.broadcasted_iota(jnp.int32, (128, 1), 0)
    low = c == 0

    def mixed(g, before, behind, v):
        prev = jnp.where(row == 0, before, pltpu.roll(g, 1, 0))
        nxt = jnp.where(row == 127, behind, pltpu.roll(g, 127, 0))
        m = prev * t0 + g * t1 + nxt * t2
        return (m / (1.0 + jnp.exp(-m)) * v).astype(BF)

    aa = mixed(ga, jnp.where(low, ha, gb[127:128]), jnp.where(low, gb[0:1], ha), va)
    ab = mixed(gb, jnp.where(low, ga[127:128], hb), jnp.where(low, hb, ga[0:1]), vb)
    act = jnp.concatenate([aa, ab], axis=0)
    d = lax.dot_general(act, down[...], (((1,), (1,)), ((), ())), preferred_element_type=F32)
    keep[...] = d[0:128]
    send[...] = d[128:256].astype(BF)


OFFSETS = (0, 7, 1, 6, 2, 5, 3, 4)


def mixer(meta, own, other, taps, ws, downs):
    vmem = pl.BlockSpec(memory_space=pltpu.VMEM)
    return pl.pallas_call(
        mixer_kernel,
        in_specs=[pl.BlockSpec(memory_space=pltpu.SMEM)] + [vmem] * (3 + len(ws) + len(downs)),
        out_shape=[
            jax.ShapeDtypeStruct((128, 2048), F32),
            jax.ShapeDtypeStruct((128, 2048), BF),
        ],
        scratch_shapes=[pltpu.VMEM((2048, 384), BF)],
        name="mixer", compiler_params=limit(20),
    )(meta, own, other, taps, *ws, *downs)


def body(
    queries,
    latents,
    shared_key,
    expand_weight,
    residual,
    out_weight,
    norm_gain,
    gate_weight,
    value_weight,
    conv_weight,
    down_weight,
):
    z, y, c, x = (lax.axis_index(a) for a in ("z", "y", "c", "x"))
    s = lax.axis_index(SP)
    tok = queries.shape[0]
    lat2 = jnp.concatenate([latents, swap(latents)], axis=0)
    sk2 = jnp.concatenate([shared_key, swap(shared_key)], axis=0)
    own_pos = s * tok + jnp.arange(tok, dtype=jnp.int32)
    other_pos = (s + 1 - 2 * c) * tok + jnp.arange(tok, dtype=jnp.int32)
    cos2, sin2 = tables(jnp.concatenate([own_pos, other_pos]), ROPE)
    cos, sin = cos2[:tok], sin2[:tok]
    ew = expand_weight
    expanded = jnp.dot(lat2, ew, preferred_element_type=F32).astype(BF)
    turned = rotate(sk2, cos2, sin2)
    ones = jnp.broadcast_to(
        (jnp.arange(64) == 0).astype(BF)[None, :], (2 * tok, 64)
    )
    kv = jnp.concatenate(
        [
            expanded[:, 0:128],
            turned,
            expanded[:, 256:320],
            expanded[:, 128:256],
            expanded[:, 320:384],
            ones,
        ],
        axis=1,
    )
    rot0 = NOPE_A + NOPE_B
    q = jnp.concatenate(
        [
            queries[:, 0:128],
            rotate(queries[:, rot0 : rot0 + 64], cos, sin),
            jnp.zeros((tok, 64), BF),
            rotate(queries[:, rot0 + 64 : rot0 + 128], cos, sin),
            queries[:, 128:192],
        ],
        axis=1,
    )
    nsp = Z * Y * C
    pairs = [(i, i + 1) for i in range(1, nsp - 1, 2)] + [(i, i - 1) for i in range(2, nsp, 2)]
    edge = jnp.concatenate([q, residual], axis=1)
    edge = jnp.where(c == 1, edge[tok - 1 : tok], edge[0:1])
    edge = lax.ppermute(edge, SP, pairs)
    edge = jnp.pad(edge, ((0, 15), (0, 0)))
    q = jnp.concatenate([q, edge[:, :384]], axis=0)
    halo_res = edge[:, 384:]
    ring = [(2 * i, 2 * ((i + 1) % Z)) for i in range(Z)]
    ring += [(2 * i + 1, 2 * ((i - 1) % Z) + 1) for i in range(Z)]

    def step(v):
        return lax.ppermute(v, ("z", "c"), ring)

    r1 = step(kv)
    r2 = step(r1)
    r3 = step(r2)
    r4 = step(r3[:tok])
    k_blocks = [kv, r1, swap(r1), r2, swap(r2), r3, swap(r3), r4, swap(r4)]
    gate_weight, value_weight, down_weight = lax.optimization_barrier(
        (gate_weight, value_weight, down_weight, kv)
    )[:3]

    def halves(w):
        n = w.shape[1] // 2
        return jnp.where(c == 0, w[:, :n], w[:, n:]), jnp.where(c == 0, w[:, n:], w[:, :n])

    gk, gs = halves(gate_weight)
    vk, vs = halves(value_weight)
    wk = jnp.concatenate([gk, vk], axis=1)
    wr = swap(jnp.concatenate([gs, vs], axis=1))
    w = jnp.concatenate([jnp.where(c == 0, wk, wr), jnp.where(c == 0, wr, wk)], axis=0)
    dk = down_weight.T
    dr = swap(dk)
    d0 = jnp.concatenate([jnp.where(c == 0, dk, dr), jnp.where(c == 0, dr, dk)], axis=0)
    d1 = step(d0)
    d2 = step(d1)
    d3 = step(d2)
    d4 = step(jnp.where(c == 0, d3[:32], d3[32:]))
    dk, ds = halves(jnp.concatenate([d1, d2, d3, d4], axis=0))
    d0 = jnp.concatenate([halves(d0)[0], dk, swap(ds)], axis=0)
    q_blocks = [q] + [shift(q, "y", k) for k in (1, 2, 3)]
    wf = shift(w, "y", 1)
    wb = shift(w, "y", -1)
    wo = jnp.concatenate([shift(wf[:32], "y", 1), shift(wb[32:], "y", -1)], axis=0)
    stack = jnp.concatenate([w, wb, wo, wf], axis=0)
    stack = jnp.concatenate([stack, stack], axis=0)
    w = lax.dynamic_slice_in_dim(stack, lax.rem(Y - y, Y) * 64, 256, 0)
    w = after(w, r4)
    f1, b1 = shift(w, "z", 1), shift(w, "z", -1)
    o = attend(q_blocks, k_blocks)
    parts = [o[0]] + [shift(o[k], "y", -k) for k in (1, 2, 3)]
    f1, b1 = after((f1, b1), *parts)
    f2, b2 = shift(f1, "z", 1), shift(b1, "z", -1)
    d0 = after(d0, *parts)
    df, db = shift(d0, "y", 1), shift(d0, "y", -1)
    attended = join(parts)
    heads = [attended] + [shift(attended, "x", -k) for k in (1, 2, 3)]
    f2, b2, df, db = after((f2, b2, df, db), *heads)
    f3, b3 = shift(f2, "z", 1), shift(b2, "z", -1)
    dh = jnp.concatenate([shift(df[:256], "y", 1), shift(db[256:], "y", -1)], axis=0)
    o4 = jnp.concatenate([shift(f3[:128], "z", 1), shift(b3[128:], "z", -1)], axis=0)
    ws = [w, f1, b1, f2, b2, f3, b3, o4]
    valid = jnp.where(c == 0, s > 0, s < nsp - 1).astype(jnp.int32)
    meta = jnp.stack([x, valid, z, c, y]).astype(jnp.int32)
    stream_own, normed = project(
        meta, heads, out_weight, residual, halo_res, norm_gain.reshape(1, -1)
    )
    other = swap(normed)
    taps = jnp.where(c == 0, conv_weight[:, :384], conv_weight[:, 384:])
    keep, send = mixer(meta, normed, other, taps, ws, [d0, db, dh, df])
    total = keep + swap(send).astype(F32)
    tb = total.astype(BF)
    got = []
    for k in (1, 2, 3):
        piece = lax.dynamic_slice_in_dim(tb, lax.rem(x + k, X) * 32, 32, 0)
        got.append(shift(piece, "x", k))
    mine = lax.dynamic_slice_in_dim(total, x * 32, 32, 0)
    summed = mine + got[0].astype(F32) + got[1].astype(F32) + got[2].astype(F32)
    return (stream_own.astype(F32) + summed).astype(BF)


def solution(mesh):
    split = Mesh(mesh.devices.reshape(Z, Y, C, X), SP_TP)
    placed = (
        P(SP, "x"),
        P(SP, None),
        P(SP, None),
        P(None, "x"),
        P(SP, None),
        P(),
        P(),
        P(SP, "x"),
        P(SP, "x"),
        P(None, "x"),
        P("x", SP),
    )
    return jax.shard_map(
        body, mesh=split, in_specs=placed, out_specs=P(SP_TP, None), check_vma=False
    )
```

```python
import functools

import jax
import jax.numpy as jnp
from jax import lax
from jax.experimental import pallas as pl
from jax.experimental.pallas import tpu as pltpu
from jax.sharding import Mesh
from jax.sharding import PartitionSpec as P

NOPE_A = 128
NOPE_B = 64
ROPE = 64
Z, Y, C, X = 8, 4, 2, 4
SP = ("z", "y", "c")
SP_TP = ("z", "y", "c", "x")
LOG2E = 1.4426950408889634
ROWS = 144
BF = jnp.bfloat16
F32 = jnp.float32


def limit(mib):
    return pltpu.CompilerParams(vmem_limit_bytes=mib * 1024 * 1024)


def shift(x, axis, k):
    n = lax.axis_size(axis)
    return lax.ppermute(x, axis, [(i, (i + k) % n) for i in range(n)])


def swap(x):
    return lax.ppermute(x, "c", [(0, 1), (1, 0)])


def tables(positions, width):
    half_width = width // 2
    frequency = 10000.0 ** (-jnp.arange(half_width, dtype=F32) / half_width)
    angles = positions.astype(F32)[:, None] * frequency[None, :]
    return (jnp.cos(angles), jnp.sin(angles))


def rotate(vectors, cos_table, sine_table):
    half_width = vectors.shape[-1] // 2
    a = vectors[:, :half_width].astype(F32)
    b = vectors[:, half_width:].astype(F32)
    turned = jnp.concatenate(
        [a * cos_table - b * sine_table, b * cos_table + a * sine_table], axis=1
    )
    return turned.astype(BF)


def split3(v):
    hi = v.astype(BF)
    r = v - hi.astype(F32)
    mid = r.astype(BF)
    lo = (r - mid.astype(F32)).astype(BF)
    return [hi.astype(F32), mid.astype(F32), lo.astype(F32)]


def attend_kernel(nq, nk, *refs):
    qs, ks, outs = refs[:nq], refs[nq : nq + nk], refs[nq + nk :]
    keys = jnp.concatenate([k[:, 0:256] for k in ks], axis=0)
    values = jnp.concatenate([k[:, 256:512] for k in ks], axis=0)
    cw = float((NOPE_A + ROPE) ** -0.5 * LOG2E)
    cn = float((NOPE_B + ROPE) ** -0.5 * LOG2E)
    nt = (((1,), (1,)), ((), ()))
    lane = lax.broadcasted_iota(jnp.int32, (ROWS, 128), 1)
    for q, o in zip(qs, outs):
        sw = lax.dot_general(q[:, 0:256], keys, nt, preferred_element_type=F32)
        mw = jnp.max(sw, axis=1, keepdims=True)
        pw = jnp.exp2((sw - mw) * cw).astype(BF)
        ow = jnp.dot(pw, values, preferred_element_type=F32)
        sn = lax.dot_general(q[:, 256:384], keys[:, 128:256], nt, preferred_element_type=F32)
        mn = jnp.max(sn, axis=1, keepdims=True)
        pn = jnp.exp2((sn - mn) * cn).astype(BF)
        on = jnp.dot(pn, values[:, 128:256], preferred_element_type=F32)
        lw = ow[:, 192:193]
        ln = on[:, 64:65]
        second = on / ln
        pieces = split3(mw * cw) + split3(lw) + split3(mn * cn) + split3(ln)
        for at, piece in enumerate(pieces):
            second = jnp.where(lane == 64 + at, piece, second)
        o[:, 0:128] = (ow[:, 0:128] / lw).astype(BF)
        o[:, 128:256] = second.astype(BF)


def attend(q_blocks, k_blocks):
    nq, nk = len(q_blocks), len(k_blocks)
    return pl.pallas_call(
        functools.partial(attend_kernel, nq, nk),
        out_shape=[jax.ShapeDtypeStruct((ROWS, 256), BF)] * nq,
        name="attend", compiler_params=limit(24),
    )(*q_blocks, *k_blocks)


def join_kernel(*refs):
    parts, out = refs[:-1], refs[-1]
    seconds = [p[:, 128:256].astype(F32) for p in parts]

    def stat(at):
        return [s[:, at : at + 1] + s[:, at + 1 : at + 2] + s[:, at + 2 : at + 3] for s in seconds]

    def weights(ms, ls):
        top = functools.reduce(jnp.maximum, ms)
        ws = [jnp.exp2(m - top) * l for m, l in zip(ms, ls)]
        total = functools.reduce(jnp.add, ws)
        return [w / total for w in ws]

    ww = weights(stat(64), stat(67))
    wn = weights(stat(70), stat(73))
    wide = functools.reduce(jnp.add, [w * p[:, 0:128].astype(F32) for w, p in zip(ww, parts)])
    narrow = functools.reduce(jnp.add, [w * s for w, s in zip(wn, seconds)])
    lane = lax.broadcasted_iota(jnp.int32, (ROWS, 128), 1)
    out[:, 0:128] = wide.astype(BF)
    out[:, 128:256] = jnp.where(lane < 64, narrow, 0.0).astype(BF)


def join(parts):
    return pl.pallas_call(
        join_kernel, out_shape=jax.ShapeDtypeStruct((ROWS, 256), BF), name="join", compiler_params=limit(4)
    )(*parts)


def project_kernel(meta, *refs):
    parts = refs[:X]
    out_weight, residual, halo, gain, stream_own, normed, stream = refs[X:]
    x = meta[0]
    total = None
    for k, part in enumerate(parts):
        first = pl.multiple_of(lax.rem(x + k, X) * 192, 64)
        d = jnp.dot(part[:, 0:192], out_weight[pl.ds(first, 192), :], preferred_element_type=F32)
        total = d if total is None else total + d
    res = jnp.concatenate([residual[...], halo[...]], axis=0).astype(F32)
    s = (res + total).astype(BF)
    stream[...] = s
    s = s.astype(F32)
    n = s * lax.rsqrt(jnp.mean(s * s, axis=1, keepdims=True) + 1e-06) * gain[...].astype(F32)
    row = lax.broadcasted_iota(jnp.int32, (ROWS, 1), 0)
    n = jnp.where(row < 128 + meta[1], n, 0.0)
    normed[...] = n.astype(BF)
    stream_own[...] = stream[pl.ds(pl.multiple_of(x * 32, 32), 32), :]


def project(meta, parts, out_weight, residual, halo, gain):
    vmem = pl.BlockSpec(memory_space=pltpu.VMEM)
    return pl.pallas_call(
        project_kernel,
        in_specs=[pl.BlockSpec(memory_space=pltpu.SMEM)] + [vmem] * 8,
        out_shape=[
            jax.ShapeDtypeStruct((32, 2048), BF),
            jax.ShapeDtypeStruct((ROWS, 2048), BF),
        ],
        scratch_shapes=[pltpu.VMEM((ROWS, 2048), BF)],
        name="project", compiler_params=limit(16),
    )(meta, *parts, out_weight, residual, halo, gain)


def mixer_kernel(meta, own, other, taps, *refs):
    parts, (keep, send, gates, values, downs) = refs[:-5], refs[-5:]
    z, c, y = meta[2], meta[3], meta[4]
    for part, off in zip(parts, OFFSETS):
        for k in range(Y):
            at = (lax.rem(z + off, Z) * Y + lax.rem(y + k, Y)) * 64
            rows = pl.ds(pl.multiple_of(at, 64), 64)
            for m, to in enumerate((gates, values, downs)):
                first = k * 192 + m * 64
                to[rows, :] = part[first : first + 64, :]
    both = jnp.concatenate([own[...], other[...]], axis=0)
    gate = jnp.dot(both, gates[...], preferred_element_type=F32).astype(BF).astype(F32)
    value = jnp.dot(both, values[...], preferred_element_type=F32).astype(BF).astype(F32)
    ga, gb = gate[0:128], gate[ROWS : ROWS + 128]
    ha, hb = gate[128:129], gate[ROWS + 128 : ROWS + 129]
    va, vb = value[0:128], value[ROWS : ROWS + 128]
    t0 = taps[0:1, :].astype(F32)
    t1 = taps[1:2, :].astype(F32)
    t2 = taps[2:3, :].astype(F32)
    row = lax.broadcasted_iota(jnp.int32, (128, 1), 0)
    low = c == 0

    def mixed(g, before, behind, v):
        prev = jnp.where(row == 0, before, pltpu.roll(g, 1, 0))
        nxt = jnp.where(row == 127, behind, pltpu.roll(g, 127, 0))
        m = prev * t0 + g * t1 + nxt * t2
        return (m / (1.0 + jnp.exp(-m)) * v).astype(BF)

    aa = mixed(ga, jnp.where(low, ha, gb[127:128]), jnp.where(low, gb[0:1], ha), va)
    ab = mixed(gb, jnp.where(low, ga[127:128], hb), jnp.where(low, hb, ga[0:1]), vb)
    act = jnp.concatenate([aa, ab], axis=0)
    d = lax.dot_general(act, downs[...], (((1,), (1,)), ((), ())), preferred_element_type=F32)
    keep[...] = d[0:128]
    send[...] = d[128:256].astype(BF)


OFFSETS = (0, 7, 1, 6, 2, 5, 3, 4)


def mixer(meta, own, other, taps, parts):
    vmem = pl.BlockSpec(memory_space=pltpu.VMEM)
    return pl.pallas_call(
        mixer_kernel,
        in_specs=[pl.BlockSpec(memory_space=pltpu.SMEM)] + [vmem] * (3 + len(parts)),
        out_shape=[
            jax.ShapeDtypeStruct((128, 2048), F32),
            jax.ShapeDtypeStruct((128, 2048), BF),
        ],
        scratch_shapes=[pltpu.VMEM((2048, 384), BF)] * 3,
        name="mixer",
        compiler_params=limit(20),
    )(meta, own, other, taps, *parts)


def body(
    queries,
    latents,
    shared_key,
    expand_weight,
    residual,
    out_weight,
    norm_gain,
    gate_weight,
    value_weight,
    conv_weight,
    down_weight,
):
    z, y, c, x = (lax.axis_index(a) for a in ("z", "y", "c", "x"))
    s = lax.axis_index(SP)
    tok = queries.shape[0]
    lat2 = jnp.concatenate([latents, swap(latents)], axis=0)
    sk2 = jnp.concatenate([shared_key, swap(shared_key)], axis=0)
    own_pos = s * tok + jnp.arange(tok, dtype=jnp.int32)
    other_pos = (s + 1 - 2 * c) * tok + jnp.arange(tok, dtype=jnp.int32)
    cos2, sin2 = tables(jnp.concatenate([own_pos, other_pos]), ROPE)
    cos, sin = cos2[:tok], sin2[:tok]
    ew = expand_weight
    expanded = jnp.dot(lat2, ew, preferred_element_type=F32).astype(BF)
    turned = rotate(sk2, cos2, sin2)
    ones = jnp.broadcast_to(
        (jnp.arange(64) == 0).astype(BF)[None, :], (2 * tok, 64)
    )
    kv = jnp.concatenate(
        [
            expanded[:, 0:128],
            turned,
            expanded[:, 256:320],
            expanded[:, 128:256],
            expanded[:, 320:384],
            ones,
        ],
        axis=1,
    )
    rot0 = NOPE_A + NOPE_B
    q = jnp.concatenate(
        [
            queries[:, 0:128],
            rotate(queries[:, rot0 : rot0 + 64], cos, sin),
            jnp.zeros((tok, 64), BF),
            rotate(queries[:, rot0 + 64 : rot0 + 128], cos, sin),
            queries[:, 128:192],
        ],
        axis=1,
    )
    nsp = Z * Y * C
    pairs = [(i, i + 1) for i in range(1, nsp - 1, 2)] + [(i, i - 1) for i in range(2, nsp, 2)]
    edge = jnp.concatenate([q, residual], axis=1)
    edge = jnp.where(c == 1, edge[tok - 1 : tok], edge[0:1])
    edge = lax.ppermute(edge, SP, pairs)
    edge = jnp.pad(edge, ((0, 15), (0, 0)))
    q = jnp.concatenate([q, edge[:, :384]], axis=0)
    halo_res = edge[:, 384:]
    ring = [(2 * i, 2 * ((i + 1) % Z)) for i in range(Z)]
    ring += [(2 * i + 1, 2 * ((i - 1) % Z) + 1) for i in range(Z)]

    def step(v):
        return lax.ppermute(v, ("z", "c"), ring)

    r1 = step(kv)
    mats = (gate_weight, value_weight, down_weight.T)
    lo = jnp.concatenate([m[:, :384] for m in mats], axis=0)
    hi = jnp.concatenate([m[:, 384:] for m in mats], axis=0)
    wk = jnp.where(c == 0, lo, hi)
    wr = swap(jnp.where(c == 0, hi, lo))
    wa, wb = jnp.where(c == 0, wk, wr), jnp.where(c == 0, wr, wk)
    w = jnp.concatenate([v[32 * m : 32 * m + 32] for m in range(3) for v in (wa, wb)], axis=0)
    qw = jnp.concatenate([q, w], axis=0)
    got = [qw] + [shift(qw, "y", k) for k in (1, 2, 3)]
    q_blocks = [v[:ROWS] for v in got]
    w = jnp.concatenate([got[-k % Y][ROWS:] for k in range(Y)], axis=0)
    r2 = step(r1)
    r3 = step(r2)
    r4 = step(r3[:tok])
    k_blocks = [kv, r1, swap(r1), r2, swap(r2), r3, swap(r3)]
    k_blocks += [r4, swap(r4)]
    f1, b1 = shift(w, "z", 1), shift(w, "z", -1)
    f2, b2 = shift(f1, "z", 1), shift(b1, "z", -1)
    f3, b3 = shift(f2, "z", 1), shift(b2, "z", -1)
    o4 = jnp.concatenate([shift(f3[:384], "z", 1), shift(b3[384:], "z", -1)], axis=0)
    ws = [w, f1, b1, f2, b2, f3, b3, o4]
    o = attend(q_blocks, k_blocks)
    parts = [o[0]] + [shift(o[k], "y", -k) for k in (1, 2, 3)]
    attended = join(parts)
    heads = [attended] + [shift(attended, "x", -k) for k in (1, 2, 3)]
    valid = jnp.where(c == 0, s > 0, s < nsp - 1).astype(jnp.int32)
    meta = jnp.stack([x, valid, z, c, y]).astype(jnp.int32)
    stream_own, normed = project(
        meta, heads, out_weight, residual, halo_res, norm_gain.reshape(1, -1)
    )
    other = swap(normed)
    taps = jnp.where(c == 0, conv_weight[:, :384], conv_weight[:, 384:])
    keep, send = mixer(meta, normed, other, taps, ws)
    total = keep + swap(send).astype(F32)
    tb = total.astype(BF)
    got = []
    for k in (1, 2, 3):
        piece = lax.dynamic_slice_in_dim(tb, lax.rem(x + k, X) * 32, 32, 0)
        got.append(shift(piece, "x", k))
    mine = lax.dynamic_slice_in_dim(total, x * 32, 32, 0)
    summed = mine + got[0].astype(F32) + got[1].astype(F32) + got[2].astype(F32)
    return (stream_own.astype(F32) + summed).astype(BF)


def solution(mesh):
    split = Mesh(mesh.devices.reshape(Z, Y, C, X), SP_TP)
    placed = (
        P(SP, "x"),
        P(SP, None),
        P(SP, None),
        P(None, "x"),
        P(SP, None),
        P(),
        P(),
        P(SP, "x"),
        P(SP, "x"),
        P(None, "x"),
        P("x", SP),
    )

    return jax.shard_map(
        body, mesh=split, in_specs=placed, out_specs=P(SP_TP, None), check_vma=False
    )
```

```python
import functools

import jax
import jax.numpy as jnp
from jax import lax
from jax.experimental import pallas as pl
from jax.experimental.pallas import tpu as pltpu
from jax.sharding import Mesh
from jax.sharding import PartitionSpec as P

NOPE_A = 128
NOPE_B = 64
ROPE = 64
Z, Y, C, X = 8, 4, 2, 4
SP = ("z", "y", "c")
SP_TP = ("z", "y", "c", "x")
LOG2E = 1.4426950408889634
MSG = 352
ROWS = 144
BF = jnp.bfloat16
F32 = jnp.float32


def limit(mib):
    return pltpu.CompilerParams(vmem_limit_bytes=mib * 1024 * 1024)


def shift(x, axis, k):
    n = lax.axis_size(axis)
    return lax.ppermute(x, axis, [(i, (i + k) % n) for i in range(n)])


def swap(x):
    return lax.ppermute(x, "c", [(0, 1), (1, 0)])


def tables(positions, width):
    half_width = width // 2
    frequency = 10000.0 ** (-jnp.arange(half_width, dtype=F32) / half_width)
    angles = positions.astype(F32)[None, :] * frequency[:, None]
    return (jnp.cos(angles), jnp.sin(angles))


def turn(a, b, cos, sin):
    return [a * cos - b * sin, b * cos + a * sin]


VM = pl.BlockSpec(memory_space=pltpu.VMEM)
SM = pl.BlockSpec(memory_space=pltpu.SMEM)


def pack_kernel(lat, down, key, out):
    out[0:128, :] = lat[...]
    out[128:160, :] = down[:, 0:512]
    out[160:176, 0:256] = down[0:16, 512:768]
    out[160:176, 256:512] = down[16:32, 512:768]
    for i in range(4):
        out[176:192, 128 * i : 128 * i + 128] = key[16 * i : 16 * i + 16, :]


def pack(lat, down, key):
    return pl.pallas_call(
        pack_kernel,
        in_specs=[VM] * 3,
        out_shape=jax.ShapeDtypeStruct((192, 512), BF),
        name="pack",
        compiler_params=limit(4),
    )(lat, down, key)


def expand_kernel(own, other, weight, cos, sin, out):
    lane = lax.broadcasted_iota(jnp.int32, (128, 128), 1)
    tail = jnp.where(lane == 64, 1.0, 0.0)
    for m, kv, down, at in ((own, 0, 128, 0), (other, 224, 176, 128)):
        e = jnp.dot(m[0:128, :], weight[...], preferred_element_type=F32).astype(BF)
        key = [m[176:192, 128 * i : 128 * i + 128].astype(F32) for i in range(4)]
        a, b = jnp.concatenate(key[:2], axis=0), jnp.concatenate(key[2:], axis=0)
        turned = turn(a, b, cos[:, at : at + 128], sin[:, at : at + 128])
        turned = jnp.concatenate(turned + [jnp.zeros((64, 128), F32)], axis=0).T
        narrow = pltpu.roll(e[:, 256:384].astype(F32), 64, 1)
        rows = slice(kv, kv + 128)
        out[rows, 0:128] = e[:, 0:128]
        out[rows, 128:256] = jnp.where(lane < 64, turned, narrow).astype(BF)
        out[rows, 256:384] = e[:, 128:256]
        out[rows, 384:512] = jnp.where(lane < 64, narrow, tail).astype(BF)
        out[down : down + 48, :] = m[128:176, :]


def expand(own, other, weight, cos, sin):
    return pl.pallas_call(
        expand_kernel,
        in_specs=[VM] * 5,
        out_shape=jax.ShapeDtypeStruct((MSG, 512), BF),
        name="expand",
        compiler_params=limit(6),
    )(own, other, weight, cos, sin)


def queries_kernel(meta, q, cos, sin, gate, value, out, edge, keep, send):
    c = meta[3]
    f = q[...].astype(F32)
    co, si = cos[:, 0:128], sin[:, 0:128]
    wide = turn(f[192:224], f[224:256], co, si) + [jnp.zeros((64, 128), F32)]
    narrow = turn(f[256:288], f[288:320], co, si) + [f[128:192]]
    tiles = [f[0:128].T, jnp.concatenate(wide, axis=0).T, jnp.concatenate(narrow, axis=0).T]
    row = lax.broadcasted_iota(jnp.int32, (128, 128), 0)
    for i, tile in enumerate(tiles):
        at = slice(128 * i, 128 * i + 128)
        out[:, at] = tile.astype(BF)
        line = jnp.sum(jnp.where(row == 127 * c, tile, 0.0), axis=0, keepdims=True)
        edge[:, at] = line.astype(BF)

    def halves(mine, others):
        for i, m in enumerate((gate, value)):
            keep[32 * i : 32 * i + 32, :] = m[:, mine]
            send[32 * i : 32 * i + 32, :] = m[:, others]

    pl.when(c == 0)(lambda: halves(slice(0, 384), slice(384, 768)))
    pl.when(c == 1)(lambda: halves(slice(384, 768), slice(0, 384)))


def turned_queries(meta, q, cos, sin, gate, value):
    return pl.pallas_call(
        queries_kernel,
        in_specs=[SM] + [VM] * 5,
        out_shape=[
            jax.ShapeDtypeStruct((128, 384), BF),
            jax.ShapeDtypeStruct((1, 384), BF),
            jax.ShapeDtypeStruct((64, 384), BF),
            jax.ShapeDtypeStruct((64, 384), BF),
        ],
        name="queries",
        compiler_params=limit(6),
    )(meta, q, cos, sin, gate, value)


def lay_kernel(meta, q, edge, keep, got, out):
    c = meta[3]
    out[0:128, :] = q[...]
    row = lax.broadcasted_iota(jnp.int32, (16, 384), 0)
    out[128:144, :] = jnp.where(row == 0, edge[...].astype(F32), 0.0).astype(BF)
    for i in range(2):
        at = ROWS + 64 * i
        rows = slice(32 * i, 32 * i + 32)
        out[pl.ds(pl.multiple_of(at + 32 * c, 16), 32), :] = keep[rows, :]
        out[pl.ds(pl.multiple_of(at + 32 - 32 * c, 16), 32), :] = got[rows, :]


def lay(meta, q, edge, keep, got):
    return pl.pallas_call(
        lay_kernel,
        in_specs=[SM] + [VM] * 4,
        out_shape=jax.ShapeDtypeStruct((ROWS + 128, 384), BF),
        name="lay",
        compiler_params=limit(4),
    )(meta, q, edge, keep, got)


def lay_down_kernel(meta, *refs):
    parts, out = refs[:-1], refs[-1]
    z, c = meta[2], meta[3]

    def lay_all(mine):
        def put(ref, at, zz, core):
            first = lax.rem(zz + 2 * Z, Z) * 64 + 32 * core
            top = pl.ds(pl.multiple_of(first, 16), 16)
            low = pl.ds(pl.multiple_of(first + 16, 16), 16)
            if mine == 0:
                out[top, :] = ref[at : at + 16, 0:384]
                out[low, :] = ref[at + 16 : at + 32, 0:384]
            else:
                out[top, 0:128] = ref[at : at + 16, 384:512]
                out[low, 0:128] = ref[at + 16 : at + 32, 384:512]
                out[top, 128:384] = ref[at + 32 : at + 48, 0:256]
                out[low, 128:384] = ref[at + 32 : at + 48, 256:512]

        sign = 2 * mine - 1
        put(parts[0], 128, z, mine)
        put(parts[0], 176, z, 1 - mine)
        for k in (1, 2, 3):
            put(parts[k], 128, z + sign * k, mine)
            put(parts[k], 176, z + sign * k, 1 - mine)
            put(parts[4 + k], 128, z - sign * k, 1 - mine)
            put(parts[4 + k], 176, z - sign * k, mine)
        put(parts[4], 128, z + 4, mine)
        put(parts[8], 128, z + 4, 1 - mine)

    pl.when(c == 0)(lambda: lay_all(0))
    pl.when(c == 1)(lambda: lay_all(1))


def lay_down(meta, parts):
    return pl.pallas_call(
        lay_down_kernel,
        in_specs=[SM] + [VM] * len(parts),
        out_shape=jax.ShapeDtypeStruct((512, 384), BF),
        name="lay_down",
        compiler_params=limit(4),
    )(meta, *parts)


def split3(v):
    hi = v.astype(BF)
    r = v - hi.astype(F32)
    mid = r.astype(BF)
    lo = (r - mid.astype(F32)).astype(BF)
    return [hi.astype(F32), mid.astype(F32), lo.astype(F32)]


def attend_kernel(nq, nk, *refs):
    qs, ks, outs = refs[:nq], refs[nq : nq + nk], refs[nq + nk :]
    spans = [(k, at) for k in ks for at in ((0, 224) if k.shape[0] == MSG else (0,))]
    keys = jnp.concatenate([k[at : at + 128, 0:256] for k, at in spans], axis=0)
    values = jnp.concatenate([k[at : at + 128, 256:512] for k, at in spans], axis=0)
    cw = float((NOPE_A + ROPE) ** -0.5 * LOG2E)
    cn = float((NOPE_B + ROPE) ** -0.5 * LOG2E)
    nt = (((1,), (1,)), ((), ()))
    lane = lax.broadcasted_iota(jnp.int32, (ROWS, 128), 1)
    for q, o in zip(qs, outs):
        sw = lax.dot_general(q[0:ROWS, 0:256], keys, nt, preferred_element_type=F32)
        mw = jnp.max(sw, axis=1, keepdims=True)
        pw = jnp.exp2((sw - mw) * cw).astype(BF)
        ow = jnp.dot(pw, values, preferred_element_type=F32)
        sn = lax.dot_general(q[0:ROWS, 256:384], keys[:, 128:256], nt, preferred_element_type=F32)
        mn = jnp.max(sn, axis=1, keepdims=True)
        pn = jnp.exp2((sn - mn) * cn).astype(BF)
        on = jnp.dot(pn, values[:, 128:256], preferred_element_type=F32)
        lw = ow[:, 192:193]
        ln = on[:, 64:65]
        second = on / ln
        pieces = split3(mw * cw) + split3(lw) + split3(mn * cn) + split3(ln)
        for at, piece in enumerate(pieces):
            second = jnp.where(lane == 64 + at, piece, second)
        o[:, 0:128] = (ow[:, 0:128] / lw).astype(BF)
        o[:, 128:256] = second.astype(BF)


def attend(q_blocks, k_blocks):
    nq, nk = len(q_blocks), len(k_blocks)
    return pl.pallas_call(
        functools.partial(attend_kernel, nq, nk),
        out_shape=[jax.ShapeDtypeStruct((ROWS, 256), BF)] * nq,
        name="attend", compiler_params=limit(24),
    )(*q_blocks, *k_blocks)


def join_kernel(*refs):
    parts, out = refs[:-1], refs[-1]
    seconds = [p[:, 128:256].astype(F32) for p in parts]

    def stat(at):
        return [s[:, at : at + 1] + s[:, at + 1 : at + 2] + s[:, at + 2 : at + 3] for s in seconds]

    def weights(ms, ls):
        top = functools.reduce(jnp.maximum, ms)
        ws = [jnp.exp2(m - top) * l for m, l in zip(ms, ls)]
        total = functools.reduce(jnp.add, ws)
        return [w / total for w in ws]

    ww = weights(stat(64), stat(67))
    wn = weights(stat(70), stat(73))
    wide = functools.reduce(jnp.add, [w * p[:, 0:128].astype(F32) for w, p in zip(ww, parts)])
    narrow = functools.reduce(jnp.add, [w * s for w, s in zip(wn, seconds)])
    lane = lax.broadcasted_iota(jnp.int32, (ROWS, 128), 1)
    out[:, 0:128] = wide.astype(BF)
    out[:, 128:256] = jnp.where(lane < 64, narrow, 0.0).astype(BF)


def join(parts):
    return pl.pallas_call(
        join_kernel, out_shape=jax.ShapeDtypeStruct((ROWS, 256), BF), name="join", compiler_params=limit(4)
    )(*parts)


def project_kernel(meta, *refs):
    parts = refs[:X]
    out_weight, residual, halo, gain, stream_own, normed, stream = refs[X:]
    x = meta[0]
    total = None
    for k, part in enumerate(parts):
        first = pl.multiple_of(lax.rem(x + k, X) * 192, 64)
        d = jnp.dot(part[:, 0:192], out_weight[pl.ds(first, 192), :], preferred_element_type=F32)
        total = d if total is None else total + d
    res = jnp.concatenate([residual[...], halo[...]], axis=0).astype(F32)
    s = (res + total).astype(BF)
    stream[...] = s
    s = s.astype(F32)
    n = s * lax.rsqrt(jnp.mean(s * s, axis=1, keepdims=True) + 1e-06) * gain[...].astype(F32)
    row = lax.broadcasted_iota(jnp.int32, (ROWS, 1), 0)
    n = jnp.where(row < 128 + meta[1], n, 0.0)
    normed[...] = n.astype(BF)
    stream_own[...] = stream[pl.ds(pl.multiple_of(x * 32, 32), 32), :]


def project(meta, parts, out_weight, residual, halo, gain):
    vmem = pl.BlockSpec(memory_space=pltpu.VMEM)
    return pl.pallas_call(
        project_kernel,
        in_specs=[pl.BlockSpec(memory_space=pltpu.SMEM)] + [vmem] * 8,
        out_shape=[
            jax.ShapeDtypeStruct((32, 2048), BF),
            jax.ShapeDtypeStruct((ROWS, 2048), BF),
        ],
        scratch_shapes=[pltpu.VMEM((ROWS, 2048), BF)],
        name="project", compiler_params=limit(16),
    )(meta, *parts, out_weight, residual, halo, gain)


def mixer_kernel(meta, own, other, taps, *refs):
    n = len(OFFSETS)
    parts, lower, (keep, send, gates, values, downs) = refs[:n], refs[n:-5], refs[-5:]
    z, c, y = meta[2], meta[3], meta[4]

    def place(zz, dy):
        at = (lax.rem(zz, Z) * Y + lax.rem(y + dy, Y)) * 64
        return pl.ds(pl.multiple_of(at, 64), 64)

    for part, off in zip(parts, OFFSETS):
        for k in range(Y):
            rows = place(z + off, k)
            gates[rows, :] = part[128 * k : 128 * k + 64, :]
            values[rows, :] = part[128 * k + 64 : 128 * k + 128, :]
    for part, (dy, first) in zip(lower, ((0, 0), (1, 0), (2, 0), (2, 4), (3, 0))):
        for i in range(part.shape[0] // 64):
            downs[place(first + i, dy), :] = part[64 * i : 64 * i + 64, :]
    both = jnp.concatenate([own[...], other[...]], axis=0)
    gate = jnp.dot(both, gates[...], preferred_element_type=F32).astype(BF).astype(F32)
    value = jnp.dot(both, values[...], preferred_element_type=F32).astype(BF).astype(F32)
    ga, gb = gate[0:128], gate[ROWS : ROWS + 128]
    ha, hb = gate[128:129], gate[ROWS + 128 : ROWS + 129]
    va, vb = value[0:128], value[ROWS : ROWS + 128]
    t0 = taps[0:1, :].astype(F32)
    t1 = taps[1:2, :].astype(F32)
    t2 = taps[2:3, :].astype(F32)
    row = lax.broadcasted_iota(jnp.int32, (128, 1), 0)
    low = c == 0

    def mixed(g, before, behind, v):
        prev = jnp.where(row == 0, before, pltpu.roll(g, 1, 0))
        nxt = jnp.where(row == 127, behind, pltpu.roll(g, 127, 0))
        m = prev * t0 + g * t1 + nxt * t2
        return (m / (1.0 + jnp.exp(-m)) * v).astype(BF)

    aa = mixed(ga, jnp.where(low, ha, gb[127:128]), jnp.where(low, gb[0:1], ha), va)
    ab = mixed(gb, jnp.where(low, ga[127:128], hb), jnp.where(low, hb, ga[0:1]), vb)
    act = jnp.concatenate([aa, ab], axis=0)
    d = lax.dot_general(act, downs[...], (((1,), (1,)), ((), ())), preferred_element_type=F32)
    keep[...] = d[0:128]
    send[...] = d[128:256].astype(BF)


OFFSETS = (0, 7, 1, 6, 2, 5, 3, 4)


def mixer(meta, own, other, taps, parts):
    return pl.pallas_call(
        mixer_kernel,
        in_specs=[SM] + [VM] * (3 + len(parts)),
        out_shape=[
            jax.ShapeDtypeStruct((128, 2048), F32),
            jax.ShapeDtypeStruct((128, 2048), BF),
        ],
        scratch_shapes=[pltpu.VMEM((2048, 384), BF)] * 3,
        name="mixer",
        compiler_params=limit(20),
    )(meta, own, other, taps, *parts)


def body(
    queries,
    latents,
    shared_key,
    expand_weight,
    residual,
    out_weight,
    norm_gain,
    gate_weight,
    value_weight,
    conv_weight,
    down_weight,
):
    z, y, c, x = (lax.axis_index(a) for a in ("z", "y", "c", "x"))
    s = lax.axis_index(SP)
    tok = queries.shape[0]
    nsp = Z * Y * C
    valid = jnp.where(c == 0, s > 0, s < nsp - 1).astype(jnp.int32)
    meta = jnp.stack([x, valid, z, c, y]).astype(jnp.int32)
    own_pos = s * tok + jnp.arange(tok, dtype=jnp.int32)
    other_pos = (s + 1 - 2 * c) * tok + jnp.arange(tok, dtype=jnp.int32)
    cos, sin = tables(jnp.concatenate([own_pos, other_pos]), ROPE)
    ring = [(2 * i, 2 * ((i + 1) % Z)) for i in range(Z)]
    ring += [(2 * i + 1, 2 * ((i - 1) % Z) + 1) for i in range(Z)]

    def step(v):
        return lax.ppermute(v, ("z", "c"), ring)

    packed = pack(latents, down_weight.T, shared_key.T)
    m0 = expand(packed, swap(packed), expand_weight, cos, sin)
    r1 = step(m0)
    q, edge, keep, send = turned_queries(meta, queries.T, cos, sin, gate_weight, value_weight)
    got = swap(send)
    pairs = [(i, i + 1) for i in range(1, nsp - 1, 2)] + [(i, i - 1) for i in range(2, nsp, 2)]
    line = lax.dynamic_slice_in_dim(residual, c * (tok - 1), 1, 0)
    edge = jnp.concatenate([edge, line], axis=1)
    edge = lax.ppermute(edge, SP, pairs)
    halo_res = jnp.pad(edge[:, 384:], ((0, 15), (0, 0)))
    qw = lay(meta, q, edge[:, :384], keep, got)
    y1, y3 = shift(qw, "y", 1), shift(qw, "y", -1)
    r2 = step(r1)
    r3 = step(r2)
    q2 = shift(y1[:ROWS], "y", 1)
    w2 = shift(y3[ROWS:], "y", -1)
    r4 = step(r3[:176])
    q_blocks = [qw, y1, q2, y3]
    w = jnp.concatenate([qw[ROWS:], y3[ROWS:], w2, y1[ROWS:]], axis=0)
    messages = [m0, r1, r2, r3, r4]
    messages += [swap(v) for k, v in enumerate(messages) if k > 0]
    f1, b1 = shift(w, "z", 1), shift(w, "z", -1)
    f2, b2 = shift(f1, "z", 1), shift(b1, "z", -1)
    f3, b3 = shift(f2, "z", 1), shift(b2, "z", -1)
    o4 = jnp.concatenate([shift(f3[:256], "z", 1), shift(b3[256:], "z", -1)], axis=0)
    d0 = lay_down(meta, messages)
    d1, d3 = shift(d0, "y", 1), shift(d0, "y", -1)
    da, db = shift(d1[:256], "y", 1), shift(d3[256:], "y", -1)
    ws = [w, f1, b1, f2, b2, f3, b3, o4, d0, d3, da, db, d1]
    o = attend(q_blocks, messages)
    parts = [o[0]] + [shift(o[k], "y", -k) for k in (1, 2, 3)]
    attended = join(parts)
    heads = [attended] + [shift(attended, "x", -k) for k in (1, 2, 3)]
    stream_own, normed = project(
        meta, heads, out_weight, residual, halo_res, norm_gain.reshape(1, -1)
    )
    other = swap(normed)
    taps = jnp.where(c == 0, conv_weight[:, :384], conv_weight[:, 384:])
    keep, send = mixer(meta, normed, other, taps, ws)
    total = keep + swap(send).astype(F32)
    tb = total.astype(BF)
    got = []
    for k in (1, 2, 3):
        piece = lax.dynamic_slice_in_dim(tb, lax.rem(x + k, X) * 32, 32, 0)
        got.append(shift(piece, "x", k))
    mine = lax.dynamic_slice_in_dim(total, x * 32, 32, 0)
    summed = mine + got[0].astype(F32) + got[1].astype(F32) + got[2].astype(F32)
    return (stream_own.astype(F32) + summed).astype(BF)


def solution(mesh):
    split = Mesh(mesh.devices.reshape(Z, Y, C, X), SP_TP)
    placed = (
        P(SP, "x"),
        P(SP, None),
        P(SP, None),
        P(None, "x"),
        P(SP, None),
        P(),
        P(),
        P(SP, "x"),
        P(SP, "x"),
        P(None, "x"),
        P("x", SP),
    )

    return jax.shard_map(
        body, mesh=split, in_specs=placed, out_specs=P(SP_TP, None), check_vma=False
    )
```

```python
import functools

import jax
import jax.numpy as jnp
from jax import lax
from jax.experimental import pallas as pl
from jax.experimental.pallas import tpu as pltpu
from jax.sharding import Mesh
from jax.sharding import PartitionSpec as P

NOPE_A = 128
NOPE_B = 64
ROPE = 64
Z, Y, C, X = 8, 4, 2, 4
SP = ("z", "y", "c")
SP_TP = ("z", "y", "c", "x")
LOG2E = 1.4426950408889634
MSG = 352
ROWS = 144
BF = jnp.bfloat16
F32 = jnp.float32


def limit(mib):
    return pltpu.CompilerParams(vmem_limit_bytes=mib * 1024 * 1024)


def shift(x, axis, k):
    n = lax.axis_size(axis)
    return lax.ppermute(x, axis, [(i, (i + k) % n) for i in range(n)])


def swap(x):
    return lax.ppermute(x, "c", [(0, 1), (1, 0)])


def tables(positions, width):
    half_width = width // 2
    frequency = 10000.0 ** (-jnp.arange(half_width, dtype=F32) / half_width)
    angles = positions.astype(F32)[None, :] * frequency[:, None]
    return (jnp.cos(angles), jnp.sin(angles))


def turn(a, b, cos, sin):
    return [a * cos - b * sin, b * cos + a * sin]


VM = pl.BlockSpec(memory_space=pltpu.VMEM)
SM = pl.BlockSpec(memory_space=pltpu.SMEM)


def expand_kernel(own, other, weight, cos, sin, out):
    lane = lax.broadcasted_iota(jnp.int32, (128, 128), 1)
    tail = jnp.where(lane == 64, 1.0, 0.0)
    for m, kv, down, at in ((own, 0, 128, 0), (other, 224, 176, 128)):
        e = jnp.dot(m[0:128, :], weight[...], preferred_element_type=F32).astype(BF)
        key = [m[176:192, 128 * i : 128 * i + 128].astype(F32) for i in range(4)]
        a, b = jnp.concatenate(key[:2], axis=0), jnp.concatenate(key[2:], axis=0)
        turned = turn(a, b, cos[:, at : at + 128], sin[:, at : at + 128])
        turned = jnp.concatenate(turned + [jnp.zeros((64, 128), F32)], axis=0).T
        narrow = pltpu.roll(e[:, 256:384].astype(F32), 64, 1)
        rows = slice(kv, kv + 128)
        out[rows, 0:128] = e[:, 0:128]
        out[rows, 128:256] = jnp.where(lane < 64, turned, narrow).astype(BF)
        out[rows, 256:384] = e[:, 128:256]
        out[rows, 384:512] = jnp.where(lane < 64, narrow, tail).astype(BF)
        out[down : down + 48, :] = m[128:176, :]


def expand(own, other, weight, cos, sin):
    return pl.pallas_call(
        expand_kernel,
        in_specs=[VM] * 5,
        out_shape=jax.ShapeDtypeStruct((MSG, 512), BF),
        name="expand",
        compiler_params=limit(6),
    )(own, other, weight, cos, sin)


def begin_kernel(meta, cos, sin, lat, down, key, q, gate, value, weight, *refs):
    packed, out, edge, keep, send, near = refs[:6]
    down_v, key_v, q_v, gate_v, value_v, sems = refs[6:]
    c = meta[3]
    pairs = (
        (down, down_v),
        (key, key_v),
        (lat, packed.at[pl.ds(0, 128)]),
        (q, q_v),
        (gate, gate_v),
        (value, value_v),
        (weight, near),
    )
    copies = [pltpu.make_async_copy(a, b, sems.at[i]) for i, (a, b) in enumerate(pairs)]
    for copy in copies:
        copy.start()
    copies[0].wait()
    packed[128:160, :] = down_v[:, 0:512]
    packed[160:176, 0:256] = down_v[0:16, 512:768]
    packed[160:176, 256:512] = down_v[16:32, 512:768]
    copies[1].wait()
    for i in range(4):
        packed[176:192, 128 * i : 128 * i + 128] = key_v[16 * i : 16 * i + 16, :]
    copies[3].wait()
    f = q_v[...].astype(F32)
    co, si = cos[:, 0:128], sin[:, 0:128]
    wide = turn(f[192:224], f[224:256], co, si) + [jnp.zeros((64, 128), F32)]
    narrow = turn(f[256:288], f[288:320], co, si) + [f[128:192]]
    tiles = [f[0:128].T, jnp.concatenate(wide, axis=0).T, jnp.concatenate(narrow, axis=0).T]
    row = lax.broadcasted_iota(jnp.int32, (128, 128), 0)
    for i, tile in enumerate(tiles):
        at = slice(128 * i, 128 * i + 128)
        out[:, at] = tile.astype(BF)
        line = jnp.sum(jnp.where(row == 127 * c, tile, 0.0), axis=0, keepdims=True)
        edge[:, at] = line.astype(BF)
    copies[4].wait()
    copies[5].wait()

    def halves(mine, others):
        for i, m in enumerate((gate_v, value_v)):
            keep[32 * i : 32 * i + 32, :] = m[:, mine]
            send[32 * i : 32 * i + 32, :] = m[:, others]

    pl.when(c == 0)(lambda: halves(slice(0, 384), slice(384, 768)))
    pl.when(c == 1)(lambda: halves(slice(384, 768), slice(0, 384)))
    copies[2].wait()
    copies[6].wait()


def begin(meta, cos, sin, *far):
    shapes = ((192, 512), (128, 384), (1, 384), (64, 384), (64, 384), (512, 384))
    scratch = ((32, 768), (64, 128), (320, 128), (32, 768), (32, 768))
    return pl.pallas_call(
        begin_kernel,
        in_specs=[SM, VM, VM] + [pl.BlockSpec(memory_space=pl.ANY)] * 7,
        out_shape=[jax.ShapeDtypeStruct(shape, BF) for shape in shapes],
        scratch_shapes=[pltpu.VMEM(shape, BF) for shape in scratch]
        + [pltpu.SemaphoreType.DMA((7,))],
        name="begin",
        compiler_params=limit(8),
    )(meta, cos, sin, *far)


def lay_kernel(meta, q, edge, keep, got, out):
    c = meta[3]
    out[0:128, :] = q[...]
    row = lax.broadcasted_iota(jnp.int32, (16, 384), 0)
    out[128:144, :] = jnp.where(row == 0, edge[...].astype(F32), 0.0).astype(BF)
    for i in range(2):
        at = ROWS + 64 * i
        rows = slice(32 * i, 32 * i + 32)
        out[pl.ds(pl.multiple_of(at + 32 * c, 16), 32), :] = keep[rows, :]
        out[pl.ds(pl.multiple_of(at + 32 - 32 * c, 16), 32), :] = got[rows, :]


def lay(meta, q, edge, keep, got):
    return pl.pallas_call(
        lay_kernel,
        in_specs=[SM] + [VM] * 4,
        out_shape=jax.ShapeDtypeStruct((ROWS + 128, 384), BF),
        name="lay",
        compiler_params=limit(4),
    )(meta, q, edge, keep, got)


def lay_down_kernel(meta, *refs):
    parts, out = refs[:-1], refs[-1]
    z, c = meta[2], meta[3]

    def lay_all(mine):
        def put(ref, at, zz, core):
            first = lax.rem(zz + 2 * Z, Z) * 64 + 32 * core
            top = pl.ds(pl.multiple_of(first, 16), 16)
            low = pl.ds(pl.multiple_of(first + 16, 16), 16)
            if mine == 0:
                out[top, :] = ref[at : at + 16, 0:384]
                out[low, :] = ref[at + 16 : at + 32, 0:384]
            else:
                out[top, 0:128] = ref[at : at + 16, 384:512]
                out[low, 0:128] = ref[at + 16 : at + 32, 384:512]
                out[top, 128:384] = ref[at + 32 : at + 48, 0:256]
                out[low, 128:384] = ref[at + 32 : at + 48, 256:512]

        sign = 2 * mine - 1
        put(parts[0], 128, z, mine)
        put(parts[0], 176, z, 1 - mine)
        for k in (1, 2, 3):
            put(parts[k], 128, z + sign * k, mine)
            put(parts[k], 176, z + sign * k, 1 - mine)
            put(parts[4 + k], 128, z - sign * k, 1 - mine)
            put(parts[4 + k], 176, z - sign * k, mine)
        put(parts[4], 128, z + 4, mine)
        put(parts[8], 128, z + 4, 1 - mine)

    pl.when(c == 0)(lambda: lay_all(0))
    pl.when(c == 1)(lambda: lay_all(1))


def lay_down(meta, parts):
    return pl.pallas_call(
        lay_down_kernel,
        in_specs=[SM] + [VM] * len(parts),
        out_shape=jax.ShapeDtypeStruct((512, 384), BF),
        name="lay_down",
        compiler_params=limit(4),
    )(meta, *parts)


def split3(v):
    hi = v.astype(BF)
    r = v - hi.astype(F32)
    mid = r.astype(BF)
    lo = (r - mid.astype(F32)).astype(BF)
    return [hi.astype(F32), mid.astype(F32), lo.astype(F32)]


def attend_kernel(nq, nk, *refs):
    qs, ks, outs = refs[:nq], refs[nq : nq + nk], refs[nq + nk :]
    spans = [(k, at) for k in ks for at in ((0, 224) if k.shape[0] == MSG else (0,))]
    keys = jnp.concatenate([k[at : at + 128, 0:256] for k, at in spans], axis=0)
    values = jnp.concatenate([k[at : at + 128, 256:512] for k, at in spans], axis=0)
    cw = float((NOPE_A + ROPE) ** -0.5 * LOG2E)
    cn = float((NOPE_B + ROPE) ** -0.5 * LOG2E)
    nt = (((1,), (1,)), ((), ()))
    lane = lax.broadcasted_iota(jnp.int32, (ROWS, 128), 1)
    for q, o in zip(qs, outs):
        sw = lax.dot_general(q[0:ROWS, 0:256], keys, nt, preferred_element_type=F32)
        mw = jnp.max(sw, axis=1, keepdims=True)
        pw = jnp.exp2((sw - mw) * cw).astype(BF)
        ow = jnp.dot(pw, values, preferred_element_type=F32)
        sn = lax.dot_general(q[0:ROWS, 256:384], keys[:, 128:256], nt, preferred_element_type=F32)
        mn = jnp.max(sn, axis=1, keepdims=True)
        pn = jnp.exp2((sn - mn) * cn).astype(BF)
        on = jnp.dot(pn, values[:, 128:256], preferred_element_type=F32)
        lw = ow[:, 192:193]
        ln = on[:, 64:65]
        second = on / ln
        pieces = split3(mw * cw) + split3(lw) + split3(mn * cn) + split3(ln)
        for at, piece in enumerate(pieces):
            second = jnp.where(lane == 64 + at, piece, second)
        o[:, 0:128] = (ow[:, 0:128] / lw).astype(BF)
        o[:, 128:256] = second.astype(BF)


def attend(q_blocks, k_blocks):
    nq, nk = len(q_blocks), len(k_blocks)
    return pl.pallas_call(
        functools.partial(attend_kernel, nq, nk),
        out_shape=[jax.ShapeDtypeStruct((ROWS, 256), BF)] * nq,
        name="attend", compiler_params=limit(24),
    )(*q_blocks, *k_blocks)


def join_kernel(*refs):
    parts, out = refs[:-1], refs[-1]
    seconds = [p[:, 128:256].astype(F32) for p in parts]

    def stat(at):
        return [s[:, at : at + 1] + s[:, at + 1 : at + 2] + s[:, at + 2 : at + 3] for s in seconds]

    def weights(ms, ls):
        top = functools.reduce(jnp.maximum, ms)
        ws = [jnp.exp2(m - top) * l for m, l in zip(ms, ls)]
        total = functools.reduce(jnp.add, ws)
        return [w / total for w in ws]

    ww = weights(stat(64), stat(67))
    wn = weights(stat(70), stat(73))
    wide = functools.reduce(jnp.add, [w * p[:, 0:128].astype(F32) for w, p in zip(ww, parts)])
    narrow = functools.reduce(jnp.add, [w * s for w, s in zip(wn, seconds)])
    lane = lax.broadcasted_iota(jnp.int32, (ROWS, 128), 1)
    out[:, 0:128] = wide.astype(BF)
    out[:, 128:256] = jnp.where(lane < 64, narrow, 0.0).astype(BF)


def join(parts):
    return pl.pallas_call(
        join_kernel, out_shape=jax.ShapeDtypeStruct((ROWS, 256), BF), name="join", compiler_params=limit(4)
    )(*parts)


def project_kernel(meta, *refs):
    parts = refs[:X]
    out_weight, residual, halo, gain, stream_own, normed, stream = refs[X:]
    x = meta[0]
    total = None
    for k, part in enumerate(parts):
        first = pl.multiple_of(lax.rem(x + k, X) * 192, 64)
        d = jnp.dot(part[:, 0:192], out_weight[pl.ds(first, 192), :], preferred_element_type=F32)
        total = d if total is None else total + d
    res = jnp.concatenate([residual[...], halo[...]], axis=0).astype(F32)
    s = (res + total).astype(BF)
    stream[...] = s
    s = s.astype(F32)
    n = s * lax.rsqrt(jnp.mean(s * s, axis=1, keepdims=True) + 1e-06) * gain[...].astype(F32)
    row = lax.broadcasted_iota(jnp.int32, (ROWS, 1), 0)
    n = jnp.where(row < 128 + meta[1], n, 0.0)
    normed[...] = n.astype(BF)
    stream_own[...] = stream[pl.ds(pl.multiple_of(x * 32, 32), 32), :]


def project(meta, parts, out_weight, residual, halo, gain):
    vmem = pl.BlockSpec(memory_space=pltpu.VMEM)
    return pl.pallas_call(
        project_kernel,
        in_specs=[pl.BlockSpec(memory_space=pltpu.SMEM)] + [vmem] * 8,
        out_shape=[
            jax.ShapeDtypeStruct((32, 2048), BF),
            jax.ShapeDtypeStruct((ROWS, 2048), BF),
        ],
        scratch_shapes=[pltpu.VMEM((ROWS, 2048), BF)],
        name="project", compiler_params=limit(16),
    )(meta, *parts, out_weight, residual, halo, gain)


def mixer_kernel(meta, own, other, taps, *refs):
    n = len(OFFSETS)
    parts, lower, (keep, send, gates, values, downs) = refs[:n], refs[n:-5], refs[-5:]
    z, c, y = meta[2], meta[3], meta[4]

    def place(zz, dy):
        at = (lax.rem(zz, Z) * Y + lax.rem(y + dy, Y)) * 64
        return pl.ds(pl.multiple_of(at, 64), 64)

    for part, off in zip(parts, OFFSETS):
        for k in range(Y):
            rows = place(z + off, k)
            gates[rows, :] = part[128 * k : 128 * k + 64, :]
            values[rows, :] = part[128 * k + 64 : 128 * k + 128, :]
    for part, (dy, first) in zip(lower, ((0, 0), (1, 0), (2, 0), (2, 4), (3, 0))):
        for i in range(part.shape[0] // 64):
            downs[place(first + i, dy), :] = part[64 * i : 64 * i + 64, :]
    both = jnp.concatenate([own[...], other[...]], axis=0)
    gate = jnp.dot(both, gates[...], preferred_element_type=F32).astype(BF).astype(F32)
    value = jnp.dot(both, values[...], preferred_element_type=F32).astype(BF).astype(F32)
    ga, gb = gate[0:128], gate[ROWS : ROWS + 128]
    ha, hb = gate[128:129], gate[ROWS + 128 : ROWS + 129]
    va, vb = value[0:128], value[ROWS : ROWS + 128]
    t0 = taps[0:1, :].astype(F32)
    t1 = taps[1:2, :].astype(F32)
    t2 = taps[2:3, :].astype(F32)
    row = lax.broadcasted_iota(jnp.int32, (128, 1), 0)
    low = c == 0

    def mixed(g, before, behind, v):
        prev = jnp.where(row == 0, before, pltpu.roll(g, 1, 0))
        nxt = jnp.where(row == 127, behind, pltpu.roll(g, 127, 0))
        m = prev * t0 + g * t1 + nxt * t2
        return (m / (1.0 + jnp.exp(-m)) * v).astype(BF)

    aa = mixed(ga, jnp.where(low, ha, gb[127:128]), jnp.where(low, gb[0:1], ha), va)
    ab = mixed(gb, jnp.where(low, ga[127:128], hb), jnp.where(low, hb, ga[0:1]), vb)
    act = jnp.concatenate([aa, ab], axis=0)
    d = lax.dot_general(act, downs[...], (((1,), (1,)), ((), ())), preferred_element_type=F32)
    keep[...] = d[0:128]
    send[...] = d[128:256].astype(BF)


OFFSETS = (0, 7, 1, 6, 2, 5, 3, 4)


def mixer(meta, own, other, taps, parts):
    return pl.pallas_call(
        mixer_kernel,
        in_specs=[SM] + [VM] * (3 + len(parts)),
        out_shape=[
            jax.ShapeDtypeStruct((128, 2048), F32),
            jax.ShapeDtypeStruct((128, 2048), BF),
        ],
        scratch_shapes=[pltpu.VMEM((2048, 384), BF)] * 3,
        name="mixer",
        compiler_params=limit(20),
    )(meta, own, other, taps, *parts)


def body(
    queries,
    latents,
    shared_key,
    expand_weight,
    residual,
    out_weight,
    norm_gain,
    gate_weight,
    value_weight,
    conv_weight,
    down_weight,
):
    z, y, c, x = (lax.axis_index(a) for a in ("z", "y", "c", "x"))
    s = lax.axis_index(SP)
    tok = queries.shape[0]
    nsp = Z * Y * C
    valid = jnp.where(c == 0, s > 0, s < nsp - 1).astype(jnp.int32)
    meta = jnp.stack([x, valid, z, c, y]).astype(jnp.int32)
    own_pos = s * tok + jnp.arange(tok, dtype=jnp.int32)
    other_pos = (s + 1 - 2 * c) * tok + jnp.arange(tok, dtype=jnp.int32)
    cos, sin = tables(jnp.concatenate([own_pos, other_pos]), ROPE)
    ring = [(2 * i, 2 * ((i + 1) % Z)) for i in range(Z)]
    ring += [(2 * i + 1, 2 * ((i - 1) % Z) + 1) for i in range(Z)]

    def step(v):
        return lax.ppermute(v, ("z", "c"), ring)

    packed, q, edge, keep, send, near = begin(
        meta,
        cos,
        sin,
        latents,
        down_weight.T,
        shared_key.T,
        queries.T,
        gate_weight,
        value_weight,
        expand_weight,
    )
    m0 = expand(packed, swap(packed), near, cos, sin)
    r1 = step(m0)
    got = swap(send)
    pairs = [(i, i + 1) for i in range(1, nsp - 1, 2)] + [(i, i - 1) for i in range(2, nsp, 2)]
    line = lax.dynamic_slice_in_dim(residual, c * (tok - 1), 1, 0)
    edge = jnp.concatenate([edge, line], axis=1)
    edge = lax.ppermute(edge, SP, pairs)
    halo_res = jnp.pad(edge[:, 384:], ((0, 15), (0, 0)))
    qw = lay(meta, q, edge[:, :384], keep, got)
    y1, y3 = shift(qw, "y", 1), shift(qw, "y", -1)
    r2 = step(r1)
    r3 = step(r2)
    q2 = shift(y1[:ROWS], "y", 1)
    w2 = shift(y3[ROWS:], "y", -1)
    r4 = step(r3[:176])
    q_blocks = [qw, y1, q2, y3]
    w = jnp.concatenate([qw[ROWS:], y3[ROWS:], w2, y1[ROWS:]], axis=0)
    messages = [m0, r1, r2, r3, r4]
    messages += [swap(v) for k, v in enumerate(messages) if k > 0]
    f1, b1 = shift(w, "z", 1), shift(w, "z", -1)
    f2, b2 = shift(f1, "z", 1), shift(b1, "z", -1)
    f3, b3 = shift(f2, "z", 1), shift(b2, "z", -1)
    o4 = jnp.concatenate([shift(f3[:256], "z", 1), shift(b3[256:], "z", -1)], axis=0)
    d0 = lay_down(meta, messages)
    d1, d3 = shift(d0, "y", 1), shift(d0, "y", -1)
    da, db = shift(d1[:256], "y", 1), shift(d3[256:], "y", -1)
    ws = [w, f1, b1, f2, b2, f3, b3, o4, d0, d3, da, db, d1]
    o = attend(q_blocks, messages)
    parts = [o[0]] + [shift(o[k], "y", -k) for k in (1, 2, 3)]
    attended = join(parts)
    heads = [attended] + [shift(attended, "x", -k) for k in (1, 2, 3)]
    stream_own, normed = project(
        meta, heads, out_weight, residual, halo_res, norm_gain.reshape(1, -1)
    )
    other = swap(normed)
    taps = jnp.where(c == 0, conv_weight[:, :384], conv_weight[:, 384:])
    keep, send = mixer(meta, normed, other, taps, ws)
    total = keep + swap(send).astype(F32)
    tb = total.astype(BF)
    got = []
    for k in (1, 2, 3):
        piece = lax.dynamic_slice_in_dim(tb, lax.rem(x + k, X) * 32, 32, 0)
        got.append(shift(piece, "x", k))
    mine = lax.dynamic_slice_in_dim(total, x * 32, 32, 0)
    summed = mine + got[0].astype(F32) + got[1].astype(F32) + got[2].astype(F32)
    return (stream_own.astype(F32) + summed).astype(BF)


def solution(mesh):
    split = Mesh(mesh.devices.reshape(Z, Y, C, X), SP_TP)
    placed = (
        P(SP, "x"),
        P(SP, None),
        P(SP, None),
        P(None, "x"),
        P(SP, None),
        P(),
        P(),
        P(SP, "x"),
        P(SP, "x"),
        P(None, "x"),
        P("x", SP),
    )

    return jax.shard_map(
        body, mesh=split, in_specs=placed, out_specs=P(SP_TP, None), check_vma=False
    )
```

```python
import functools

import jax
import jax.numpy as jnp
from jax import lax
from jax.experimental import pallas as pl
from jax.experimental.pallas import tpu as pltpu
from jax.sharding import Mesh
from jax.sharding import PartitionSpec as P

NOPE_A = 128
NOPE_B = 64
ROPE = 64
Z, Y, C, X = 8, 4, 2, 4
SP = ("z", "y", "c")
SP_TP = ("z", "y", "c", "x")
LOG2E = 1.4426950408889634
MSG = 352
ROWS = 144
BF = jnp.bfloat16
F32 = jnp.float32


def limit(mib):
    return pltpu.CompilerParams(vmem_limit_bytes=mib * 1024 * 1024)


def shift(x, axis, k):
    n = lax.axis_size(axis)
    return lax.ppermute(x, axis, [(i, (i + k) % n) for i in range(n)])


def swap(x):
    return lax.ppermute(x, "c", [(0, 1), (1, 0)])


def tables(positions, width):
    half_width = width // 2
    frequency = 10000.0 ** (-jnp.arange(half_width, dtype=F32) / half_width)
    angles = positions.astype(F32)[None, :] * frequency[:, None]
    return (jnp.cos(angles), jnp.sin(angles))


def turn(a, b, cos, sin):
    return [a * cos - b * sin, b * cos + a * sin]


VM = pl.BlockSpec(memory_space=pltpu.VMEM)
SM = pl.BlockSpec(memory_space=pltpu.SMEM)


def expand_kernel(own, other, weight, cos, sin, out):
    lane = lax.broadcasted_iota(jnp.int32, (128, 128), 1)
    tail = jnp.where(lane == 64, 1.0, 0.0)
    for m, kv, down, at in ((own, 0, 128, 0), (other, 224, 176, 128)):
        e = jnp.dot(m[0:128, :], weight[...], preferred_element_type=F32).astype(BF)
        key = [m[176:192, 128 * i : 128 * i + 128].astype(F32) for i in range(4)]
        a, b = jnp.concatenate(key[:2], axis=0), jnp.concatenate(key[2:], axis=0)
        turned = turn(a, b, cos[:, at : at + 128], sin[:, at : at + 128])
        turned = jnp.concatenate(turned + [jnp.zeros((64, 128), F32)], axis=0).T
        narrow = pltpu.roll(e[:, 256:384].astype(F32), 64, 1)
        rows = slice(kv, kv + 128)
        out[rows, 0:128] = e[:, 0:128]
        out[rows, 128:256] = jnp.where(lane < 64, turned, narrow).astype(BF)
        out[rows, 256:384] = e[:, 128:256]
        out[rows, 384:512] = jnp.where(lane < 64, narrow, tail).astype(BF)
        out[down : down + 48, :] = m[128:176, :]


def expand(own, other, weight, cos, sin):
    return pl.pallas_call(
        expand_kernel,
        in_specs=[VM] * 5,
        out_shape=jax.ShapeDtypeStruct((MSG, 512), BF),
        name="expand",
        compiler_params=limit(6),
    )(own, other, weight, cos, sin)


def begin_kernel(meta, cos, sin, lat, down, key, q, gate, value, weight, res, *refs):
    packed, out, edge, keep, send, near = refs[:6]
    down_v, key_v, q_v, gate_v, value_v, res_v, sems = refs[6:]
    c = meta[3]
    pairs = (
        (down, down_v),
        (key, key_v),
        (lat, packed.at[pl.ds(0, 128)]),
        (q, q_v),
        (gate, gate_v),
        (value, value_v),
        (weight, near),
        (res.at[pl.ds(pl.multiple_of(112 * c, 16), 16)], res_v),
    )
    copies = [pltpu.make_async_copy(a, b, sems.at[i]) for i, (a, b) in enumerate(pairs)]
    for copy in copies:
        copy.start()
    copies[0].wait()
    packed[128:160, :] = down_v[:, 0:512]
    packed[160:176, 0:256] = down_v[0:16, 512:768]
    packed[160:176, 256:512] = down_v[16:32, 512:768]
    copies[1].wait()
    for i in range(4):
        packed[176:192, 128 * i : 128 * i + 128] = key_v[16 * i : 16 * i + 16, :]
    copies[3].wait()
    f = q_v[...].astype(F32)
    co, si = cos[:, 0:128], sin[:, 0:128]
    wide = turn(f[192:224], f[224:256], co, si) + [jnp.zeros((64, 128), F32)]
    narrow = turn(f[256:288], f[288:320], co, si) + [f[128:192]]
    tiles = [f[0:128].T, jnp.concatenate(wide, axis=0).T, jnp.concatenate(narrow, axis=0).T]
    row = lax.broadcasted_iota(jnp.int32, (128, 128), 0)
    for i, tile in enumerate(tiles):
        at = slice(128 * i, 128 * i + 128)
        out[:, at] = tile.astype(BF)
        line = jnp.sum(jnp.where(row == 127 * c, tile, 0.0), axis=0, keepdims=True)
        edge[:, at] = line.astype(BF)
    copies[4].wait()
    copies[5].wait()

    def halves(mine, others):
        for i, m in enumerate((gate_v, value_v)):
            keep[32 * i : 32 * i + 32, :] = m[:, mine]
            send[32 * i : 32 * i + 32, :] = m[:, others]

    pl.when(c == 0)(lambda: halves(slice(0, 384), slice(384, 768)))
    pl.when(c == 1)(lambda: halves(slice(384, 768), slice(0, 384)))
    copies[7].wait()
    edge[:, 384:2432] = jnp.where(
        c == 1, res_v[15:16, :].astype(F32), res_v[0:1, :].astype(F32)
    ).astype(BF)
    copies[2].wait()
    copies[6].wait()


def begin(meta, cos, sin, *far):
    shapes = ((192, 512), (128, 384), (1, 2432), (64, 384), (64, 384), (512, 384))
    scratch = ((32, 768), (64, 128), (320, 128), (32, 768), (32, 768), (16, 2048))
    far = [pltpu.with_memory_space_constraint(v, pltpu.HBM) for v in far]
    return pl.pallas_call(
        begin_kernel,
        in_specs=[SM, VM, VM] + [pl.BlockSpec(memory_space=pltpu.HBM)] * 8,
        out_shape=[jax.ShapeDtypeStruct(shape, BF) for shape in shapes],
        scratch_shapes=[pltpu.VMEM(shape, BF) for shape in scratch]
        + [pltpu.SemaphoreType.DMA((8,))],
        name="begin",
        compiler_params=limit(8),
    )(meta, cos, sin, *far)


def lay_kernel(meta, q, edge, keep, got, out):
    c = meta[3]
    out[0:128, :] = q[...]
    row = lax.broadcasted_iota(jnp.int32, (16, 384), 0)
    out[128:144, :] = jnp.where(row == 0, edge[...].astype(F32), 0.0).astype(BF)
    for i in range(2):
        at = ROWS + 64 * i
        rows = slice(32 * i, 32 * i + 32)
        out[pl.ds(pl.multiple_of(at + 32 * c, 16), 32), :] = keep[rows, :]
        out[pl.ds(pl.multiple_of(at + 32 - 32 * c, 16), 32), :] = got[rows, :]


def lay(meta, q, edge, keep, got):
    return pl.pallas_call(
        lay_kernel,
        in_specs=[SM] + [VM] * 4,
        out_shape=jax.ShapeDtypeStruct((ROWS + 128, 384), BF),
        name="lay",
        compiler_params=limit(4),
    )(meta, q, edge, keep, got)


def lay_down_kernel(meta, *refs):
    parts, out = refs[:-1], refs[-1]
    z, c = meta[2], meta[3]

    def lay_all(mine):
        def put(ref, at, zz, core):
            first = lax.rem(zz + 2 * Z, Z) * 64 + 32 * core
            top = pl.ds(pl.multiple_of(first, 16), 16)
            low = pl.ds(pl.multiple_of(first + 16, 16), 16)
            if mine == 0:
                out[top, :] = ref[at : at + 16, 0:384]
                out[low, :] = ref[at + 16 : at + 32, 0:384]
            else:
                out[top, 0:128] = ref[at : at + 16, 384:512]
                out[low, 0:128] = ref[at + 16 : at + 32, 384:512]
                out[top, 128:384] = ref[at + 32 : at + 48, 0:256]
                out[low, 128:384] = ref[at + 32 : at + 48, 256:512]

        sign = 2 * mine - 1
        put(parts[0], 128, z, mine)
        put(parts[0], 176, z, 1 - mine)
        for k in (1, 2, 3):
            put(parts[k], 128, z + sign * k, mine)
            put(parts[k], 176, z + sign * k, 1 - mine)
            put(parts[4 + k], 128, z - sign * k, 1 - mine)
            put(parts[4 + k], 176, z - sign * k, mine)
        put(parts[4], 128, z + 4, mine)
        put(parts[8], 128, z + 4, 1 - mine)

    pl.when(c == 0)(lambda: lay_all(0))
    pl.when(c == 1)(lambda: lay_all(1))


def lay_down(meta, parts):
    return pl.pallas_call(
        lay_down_kernel,
        in_specs=[SM] + [VM] * len(parts),
        out_shape=jax.ShapeDtypeStruct((512, 384), BF),
        name="lay_down",
        compiler_params=limit(4),
    )(meta, *parts)


def split3(v):
    hi = v.astype(BF)
    r = v - hi.astype(F32)
    mid = r.astype(BF)
    lo = (r - mid.astype(F32)).astype(BF)
    return [hi.astype(F32), mid.astype(F32), lo.astype(F32)]


def attend_kernel(nq, nk, *refs):
    qs, ks, outs = refs[:nq], refs[nq : nq + nk], refs[nq + nk :]
    spans = [(k, at) for k in ks for at in ((0, 224) if k.shape[0] == MSG else (0,))]
    keys = jnp.concatenate([k[at : at + 128, 0:256] for k, at in spans], axis=0)
    values = jnp.concatenate([k[at : at + 128, 256:512] for k, at in spans], axis=0)
    cw = float((NOPE_A + ROPE) ** -0.5 * LOG2E)
    cn = float((NOPE_B + ROPE) ** -0.5 * LOG2E)
    nt = (((1,), (1,)), ((), ()))
    lane = lax.broadcasted_iota(jnp.int32, (ROWS, 128), 1)
    for q, o in zip(qs, outs):
        sw = lax.dot_general(q[0:ROWS, 0:256], keys, nt, preferred_element_type=F32)
        mw = jnp.max(sw, axis=1, keepdims=True)
        pw = jnp.exp2((sw - mw) * cw).astype(BF)
        ow = jnp.dot(pw, values, preferred_element_type=F32)
        sn = lax.dot_general(q[0:ROWS, 256:384], keys[:, 128:256], nt, preferred_element_type=F32)
        mn = jnp.max(sn, axis=1, keepdims=True)
        pn = jnp.exp2((sn - mn) * cn).astype(BF)
        on = jnp.dot(pn, values[:, 128:256], preferred_element_type=F32)
        lw = ow[:, 192:193]
        ln = on[:, 64:65]
        second = on / ln
        pieces = split3(mw * cw) + split3(lw) + split3(mn * cn) + split3(ln)
        for at, piece in enumerate(pieces):
            second = jnp.where(lane == 64 + at, piece, second)
        o[:, 0:128] = (ow[:, 0:128] / lw).astype(BF)
        o[:, 128:256] = second.astype(BF)


def attend(q_blocks, k_blocks):
    nq, nk = len(q_blocks), len(k_blocks)
    return pl.pallas_call(
        functools.partial(attend_kernel, nq, nk),
        out_shape=[jax.ShapeDtypeStruct((ROWS, 256), BF)] * nq,
        name="attend", compiler_params=limit(24),
    )(*q_blocks, *k_blocks)


def join_kernel(*refs):
    parts, out = refs[:-1], refs[-1]
    seconds = [p[:, 128:256].astype(F32) for p in parts]

    def stat(at):
        return [s[:, at : at + 1] + s[:, at + 1 : at + 2] + s[:, at + 2 : at + 3] for s in seconds]

    def weights(ms, ls):
        top = functools.reduce(jnp.maximum, ms)
        ws = [jnp.exp2(m - top) * l for m, l in zip(ms, ls)]
        total = functools.reduce(jnp.add, ws)
        return [w / total for w in ws]

    ww = weights(stat(64), stat(67))
    wn = weights(stat(70), stat(73))
    wide = functools.reduce(jnp.add, [w * p[:, 0:128].astype(F32) for w, p in zip(ww, parts)])
    narrow = functools.reduce(jnp.add, [w * s for w, s in zip(wn, seconds)])
    lane = lax.broadcasted_iota(jnp.int32, (ROWS, 128), 1)
    out[:, 0:128] = wide.astype(BF)
    out[:, 128:256] = jnp.where(lane < 64, narrow, 0.0).astype(BF)


def join(parts):
    return pl.pallas_call(
        join_kernel, out_shape=jax.ShapeDtypeStruct((ROWS, 256), BF), name="join", compiler_params=limit(4)
    )(*parts)


def project_kernel(meta, *refs):
    parts = refs[:X]
    out_weight, residual, halo, gain, stream_own, normed, stream = refs[X:]
    x = meta[0]
    total = None
    for k, part in enumerate(parts):
        first = pl.multiple_of(lax.rem(x + k, X) * 192, 64)
        d = jnp.dot(part[:, 0:192], out_weight[pl.ds(first, 192), :], preferred_element_type=F32)
        total = d if total is None else total + d
    res = jnp.concatenate([residual[...], halo[...]], axis=0).astype(F32)
    s = (res + total).astype(BF)
    stream[...] = s
    s = s.astype(F32)
    n = s * lax.rsqrt(jnp.mean(s * s, axis=1, keepdims=True) + 1e-06) * gain[...].astype(F32)
    row = lax.broadcasted_iota(jnp.int32, (ROWS, 1), 0)
    n = jnp.where(row < 128 + meta[1], n, 0.0)
    normed[...] = n.astype(BF)
    stream_own[...] = stream[pl.ds(pl.multiple_of(x * 32, 32), 32), :]


def project(meta, parts, out_weight, residual, halo, gain):
    vmem = pl.BlockSpec(memory_space=pltpu.VMEM)
    return pl.pallas_call(
        project_kernel,
        in_specs=[pl.BlockSpec(memory_space=pltpu.SMEM)] + [vmem] * 8,
        out_shape=[
            jax.ShapeDtypeStruct((32, 2048), BF),
            jax.ShapeDtypeStruct((ROWS, 2048), BF),
        ],
        scratch_shapes=[pltpu.VMEM((ROWS, 2048), BF)],
        name="project", compiler_params=limit(16),
    )(meta, *parts, out_weight, residual, halo, gain)


def mixer_kernel(meta, own, other, taps, *refs):
    n = len(OFFSETS)
    parts, lower, (keep, send, gates, values, downs) = refs[:n], refs[n:-5], refs[-5:]
    z, c, y = meta[2], meta[3], meta[4]

    def place(zz, dy):
        at = (lax.rem(zz, Z) * Y + lax.rem(y + dy, Y)) * 64
        return pl.ds(pl.multiple_of(at, 64), 64)

    for part, off in zip(parts, OFFSETS):
        for k in range(Y):
            rows = place(z + off, k)
            gates[rows, :] = part[128 * k : 128 * k + 64, :]
            values[rows, :] = part[128 * k + 64 : 128 * k + 128, :]
    for part, (dy, first) in zip(lower, ((0, 0), (1, 0), (2, 0), (2, 4), (3, 0))):
        for i in range(part.shape[0] // 64):
            downs[place(first + i, dy), :] = part[64 * i : 64 * i + 64, :]
    both = jnp.concatenate([own[...], other[...]], axis=0)
    gate = jnp.dot(both, gates[...], preferred_element_type=F32).astype(BF).astype(F32)
    value = jnp.dot(both, values[...], preferred_element_type=F32).astype(BF).astype(F32)
    ga, gb = gate[0:128], gate[ROWS : ROWS + 128]
    ha, hb = gate[128:129], gate[ROWS + 128 : ROWS + 129]
    va, vb = value[0:128], value[ROWS : ROWS + 128]
    t0 = taps[0:1, :].astype(F32)
    t1 = taps[1:2, :].astype(F32)
    t2 = taps[2:3, :].astype(F32)
    row = lax.broadcasted_iota(jnp.int32, (128, 1), 0)
    low = c == 0

    def mixed(g, before, behind, v):
        prev = jnp.where(row == 0, before, pltpu.roll(g, 1, 0))
        nxt = jnp.where(row == 127, behind, pltpu.roll(g, 127, 0))
        m = prev * t0 + g * t1 + nxt * t2
        return (m / (1.0 + jnp.exp(-m)) * v).astype(BF)

    aa = mixed(ga, jnp.where(low, ha, gb[127:128]), jnp.where(low, gb[0:1], ha), va)
    ab = mixed(gb, jnp.where(low, ga[127:128], hb), jnp.where(low, hb, ga[0:1]), vb)
    act = jnp.concatenate([aa, ab], axis=0)
    d = lax.dot_general(act, downs[...], (((1,), (1,)), ((), ())), preferred_element_type=F32)
    keep[...] = d[0:128]
    send[...] = d[128:256].astype(BF)


OFFSETS = (0, 7, 1, 6, 2, 5, 3, 4)


def mixer(meta, own, other, taps, parts):
    return pl.pallas_call(
        mixer_kernel,
        in_specs=[SM] + [VM] * (3 + len(parts)),
        out_shape=[
            jax.ShapeDtypeStruct((128, 2048), F32),
            jax.ShapeDtypeStruct((128, 2048), BF),
        ],
        scratch_shapes=[pltpu.VMEM((2048, 384), BF)] * 3,
        name="mixer",
        compiler_params=limit(20),
    )(meta, own, other, taps, *parts)


def body(
    queries,
    latents,
    shared_key,
    expand_weight,
    residual,
    out_weight,
    norm_gain,
    gate_weight,
    value_weight,
    conv_weight,
    down_weight,
):
    z, y, c, x = (lax.axis_index(a) for a in ("z", "y", "c", "x"))
    s = lax.axis_index(SP)
    tok = queries.shape[0]
    nsp = Z * Y * C
    valid = jnp.where(c == 0, s > 0, s < nsp - 1).astype(jnp.int32)
    meta = jnp.stack([x, valid, z, c, y]).astype(jnp.int32)
    own_pos = s * tok + jnp.arange(tok, dtype=jnp.int32)
    other_pos = (s + 1 - 2 * c) * tok + jnp.arange(tok, dtype=jnp.int32)
    cos, sin = tables(jnp.concatenate([own_pos, other_pos]), ROPE)
    ring = [(2 * i, 2 * ((i + 1) % Z)) for i in range(Z)]
    ring += [(2 * i + 1, 2 * ((i - 1) % Z) + 1) for i in range(Z)]

    def step(v):
        return lax.ppermute(v, ("z", "c"), ring)

    packed, q, edge, keep, send, near = begin(
        meta,
        cos,
        sin,
        latents,
        down_weight.T,
        shared_key.T,
        queries.T,
        gate_weight,
        value_weight,
        expand_weight,
        residual,
    )
    m0 = expand(packed, swap(packed), near, cos, sin)
    r1 = step(m0)
    got = swap(send)
    pairs = [(i, i + 1) for i in range(1, nsp - 1, 2)] + [(i, i - 1) for i in range(2, nsp, 2)]
    edge = lax.ppermute(edge, SP, pairs)
    halo_res = jnp.pad(edge[:, 384:], ((0, 15), (0, 0)))
    qw = lay(meta, q, edge[:, :384], keep, got)
    y1, y3 = shift(qw, "y", 1), shift(qw, "y", -1)
    r2 = step(r1)
    r3 = step(r2)
    q2 = shift(y1[:ROWS], "y", 1)
    w2 = shift(y3[ROWS:], "y", -1)
    r4 = step(r3[:176])
    q_blocks = [qw, y1, q2, y3]
    w = jnp.concatenate([qw[ROWS:], y3[ROWS:], w2, y1[ROWS:]], axis=0)
    messages = [m0, r1, r2, r3, r4]
    messages += [swap(v) for k, v in enumerate(messages) if k > 0]
    f1, b1 = shift(w, "z", 1), shift(w, "z", -1)
    f2, b2 = shift(f1, "z", 1), shift(b1, "z", -1)
    f3, b3 = shift(f2, "z", 1), shift(b2, "z", -1)
    o4 = jnp.concatenate([shift(f3[:256], "z", 1), shift(b3[256:], "z", -1)], axis=0)
    d0 = lay_down(meta, messages)
    d1, d3 = shift(d0, "y", 1), shift(d0, "y", -1)
    da, db = shift(d1[:256], "y", 1), shift(d3[256:], "y", -1)
    ws = [w, f1, b1, f2, b2, f3, b3, o4, d0, d3, da, db, d1]
    o = attend(q_blocks, messages)
    parts = [o[0]] + [shift(o[k], "y", -k) for k in (1, 2, 3)]
    attended = join(parts)
    heads = [attended] + [shift(attended, "x", -k) for k in (1, 2, 3)]
    stream_own, normed = project(
        meta, heads, out_weight, residual, halo_res, norm_gain.reshape(1, -1)
    )
    other = swap(normed)
    taps = jnp.where(c == 0, conv_weight[:, :384], conv_weight[:, 384:])
    keep, send = mixer(meta, normed, other, taps, ws)
    total = keep + swap(send).astype(F32)
    tb = total.astype(BF)
    got = []
    for k in (1, 2, 3):
        piece = lax.dynamic_slice_in_dim(tb, lax.rem(x + k, X) * 32, 32, 0)
        got.append(shift(piece, "x", k))
    mine = lax.dynamic_slice_in_dim(total, x * 32, 32, 0)
    summed = mine + got[0].astype(F32) + got[1].astype(F32) + got[2].astype(F32)
    return (stream_own.astype(F32) + summed).astype(BF)


def solution(mesh):
    split = Mesh(mesh.devices.reshape(Z, Y, C, X), SP_TP)
    placed = (
        P(SP, "x"),
        P(SP, None),
        P(SP, None),
        P(None, "x"),
        P(SP, None),
        P(),
        P(),
        P(SP, "x"),
        P(SP, "x"),
        P(None, "x"),
        P("x", SP),
    )

    return jax.shard_map(
        body, mesh=split, in_specs=placed, out_specs=P(SP_TP, None), check_vma=False
    )
```
